32 devices in a mesh: fs: 8 (over z, x), tp: 4 (over y, core).
Axes of the slice: x: 2, y: 2, z: 4, core: 2. Of those that a mesh axis runs over, the one named last changes fastest.
Arguments:
- tokens: bfloat16 [1024, 2048], P('fs'), may hold values from -6 to 6
- gain: float32 [2048], P('fs'), may hold values from 0.1 to 1.9
- up_master: float32 [2048, 8192], P('fs', 'tp'), may hold values from -0.125 to 0.125
- down_master: float32 [2048, 8192], P('fs', 'tp'), may hold values from -0.0625 to 0.0625
Outputs:
- up_sampled: bfloat16 [8, 2048, 1024], P('fs', None, 'tp')
- down_sampled: bfloat16 [8, 2048, 1024], P('fs', None, 'tp')
- mixed: bfloat16 [1024, 2048], P('fs', 'tp')
The draws below stay inside these ranges and needn't reach their ends.
All inputs are finite; a program needn't handle non-finite values.
Results may differ from the reference program's by a relative error of at most 0.0087.
Values may be sent and summed in bfloat16 or wider, within the bound.
A program may use at most 64 MiB of HBM per device.

```python
import jax
import jax.numpy as jnp
from jax import lax

D = 2048
FF = 8192
SUB = 8
TOKENS = 1024
UNITS_DEV = 256
N_FS = 8
N_TP = 4


def levels(stream_key, shape, split, smallest, largest):
    def one(axis_at, shards_of):
        draws = jax.random.uniform(jax.random.fold_in(jax.random.fold_in(stream_key, 6), axis_at), (shards_of,), jnp.float32, smallest / len(split), largest / len(split))
        return jnp.repeat(jnp.exp(draws), shape[axis_at] // shards_of).reshape((-1,) + (1,) * (len(shape) - axis_at - 1))

    level = one(*split[0])
    for cut in split[1:]:
        level = level * one(*cut)
    return level


def centred(stream_key, shape, width, bound, split=(), kind=jnp.bfloat16):
    drawn = width * jax.random.normal(stream_key, shape, jnp.float32)
    if split:
        drawn = drawn * levels(stream_key, shape, split, -0.22, 0.18)
    return jnp.clip(drawn, -bound, bound).astype(kind)


def setup_inputs(seed: int = 0) -> dict:
    key_list = jax.random.split(jax.random.key(seed), 5)
    tokens = centred(key_list[0], (TOKENS, D), 1.0, 6.0, ((0, 8),))
    gain = jnp.clip(1.0 + 0.18 * jax.random.normal(key_list[1], (D,), jnp.float32), 0.1, 1.9)
    up_master = centred(key_list[2], (D, FF), D ** -0.5, 0.125, ((0, 8), (1, 4)), jnp.float32)
    down_master = centred(key_list[3], (D, FF), FF ** -0.5, 0.0625, ((0, 8), (1, 4)), jnp.float32)
    return dict(tokens=tokens, gain=gain, up_master=up_master, down_master=down_master)


def sampled(weight):
    blocks = weight.reshape(D, N_TP, SUB, UNITS_DEV).transpose(2, 0, 1, 3).reshape(SUB, D, N_TP * UNITS_DEV)
    return jnp.tile(blocks, (N_FS // SUB, 1, 1))

def reference(tokens, gain, up_master, down_master):
    up_round = (gain[:, None] * up_master).astype(jnp.bfloat16)
    down_round = down_master.astype(jnp.bfloat16)
    widened = tokens.astype(jnp.float32)
    normed = (widened * lax.rsqrt(lax.optimization_barrier(jnp.mean(widened * widened, axis=1, keepdims=True)) + 1e-06)).astype(jnp.bfloat16)
    pre_units = jnp.dot(normed, up_round, preferred_element_type=jnp.float32)
    act_units = jnp.square(jax.nn.relu(pre_units)).astype(jnp.bfloat16)
    mixed = lax.dot_general(act_units, down_round, (((1,), (1,)), ((), ())), preferred_element_type=jnp.float32)
    return (sampled(up_round), sampled(down_round), mixed.astype(jnp.bfloat16))
```

```python
import functools
import types

import jax
import jax.numpy as jnp
from jax import lax
from jax.experimental import pallas as pl
from jax.experimental.pallas import tpu as pltpu
from jax.sharding import PartitionSpec as P

SUB = 8
EPS = 1e-06
BF16 = jnp.bfloat16
F32 = jnp.float32
PIECES = 4


def fused(nz, names, tok_h, gain, upm_h, dnm_h, up_h, dn_h, mix_o, *refs):
    r = types.SimpleNamespace(**dict(zip(names, refs)))
    mark = jax.named_scope
    f, t = lax.axis_index("fs"), lax.axis_index("tp")
    z, x = f // 2, f % 2
    y, c = t // 2, t % 2
    ox, oy, oc = 1 - x, 1 - y, 1 - c
    rows, width = r.tok.shape
    cols = width // nz
    feat = r.upm.shape[0]
    units = r.act.shape[1]
    fine = feat // PIECES
    wide = 2 * fine
    span = 2 * rows
    close = z // 2
    same = (z + 2) % 4
    pair = z + 1 - 2 * (z % 2)
    across = (pair + 2) % 4
    inner = 2 - close
    central = jnp.logical_or(z == 1, z == 2)
    at_x = (z * 2 + ox, t)
    at_y = (f, oy * 2 + c)
    at_c = (f, y * 2 + oc)

    def at_z(zz):
        return (zz * 2 + x, t)

    fetch = [pltpu.make_async_copy(src, dst, r.s_in.at[n]) for n, (src, dst) in enumerate(
        ((tok_h, r.tok), (upm_h, r.upm), (dnm_h, r.dnm)))]
    for copy in fetch:
        copy.start()

    barrier = pltpu.get_barrier_semaphore()
    partners = (at_z(pair), at_z(same), at_z(across), at_x, at_y, at_c)
    for dev in partners:
        pl.semaphore_signal(barrier, inc=1, device_id=dev, device_id_type=pl.DeviceIdType.MESH)

    sent = []

    def remote(src, dst, ssem, rsem, dev):
        return pltpu.make_async_remote_copy(
            src_ref=src, dst_ref=dst, send_sem=ssem, recv_sem=rsem,
            device_id=dev, device_id_type=pl.DeviceIdType.MESH)

    def send(src, dst, ssem, rsem, dev):
        copy = remote(src, dst, ssem, rsem, dev)
        copy.start()
        sent.append((copy, None))

    def prepare(src, dst, ssem, rsem, dev, when):
        copy = remote(src, dst, ssem, rsem, dev)
        sent.append((copy, when))
        return copy

    def arrived(dst, ssem, rsem, dev):
        remote(dst, dst, ssem, rsem, dev).wait_recv()

    def at_rows(ref, k):
        return ref.at[pl.ds(pl.multiple_of(k * feat, feat), feat), :]

    def at_piece(ref, k, p):
        return ref.at[pl.ds(pl.multiple_of(k * feat + p * fine, fine), fine), :]

    def cast(src, dst, out, factor):
        for m in range(SUB):
            block = src[:, m * units:(m + 1) * units]
            dst[m] = (block if factor is None else factor * block).astype(BF16)
        block = src[:, pl.ds(pl.multiple_of(f * units, units), units)]
        out[pl.ds(pl.multiple_of(f * feat, feat), feat), :] = (
            block if factor is None else factor * block).astype(BF16)

    with mark("norm"):
        fetch[0].wait()
        full = r.tok[...].astype(F32)
        scale = lax.rsqrt(jnp.mean(full * full, axis=1, keepdims=True) + EPS)
        for q in range(nz):
            r.xg[q, z, x] = (full[:, q * cols:(q + 1) * cols] * scale).astype(BF16)
    with mark("castup"):
        fetch[1].wait()
        cast(r.upm, r.up_s, r.up_o, jnp.transpose(gain[...]))
    with mark("barrier"):
        pl.semaphore_wait(barrier, len(partners))

    def token_x(zz):
        part = r.xg.at[t, zz, x]
        send(part, part, r.s_tx.at[zz], r.r_tx.at[zz], at_x)

    def token_y(zz, xx):
        part = r.xg.at[t, zz, xx]
        send(part, part, r.s_ty.at[zz, xx], r.r_ty.at[zz, xx], at_y)

    def token_c(yy, zz, xx):
        part = r.xg.at[yy * 2 + c, zz, xx]
        send(part, part, r.s_tc.at[yy, zz, xx], r.r_tc.at[yy, zz, xx], at_c)

    def up_x(zz):
        send(r.up_s.at[zz * 2 + ox], r.up_r.at[zz], r.s_ux.at[zz], r.r_ux.at[zz], at_x)

    def up_own(zz):
        send(r.up_s.at[zz * 2 + x], at_rows(r.up_o, f), r.s_up.at[zz], r.r_up.at[f], at_z(zz))

    def up_relay(zz):
        arrived(r.up_r.at[zz], r.s_ux.at[zz], r.r_ux.at[zz], at_x)
        send(r.up_r.at[zz], at_rows(r.up_o, z * 2 + ox), r.s_ur.at[zz], r.r_up.at[z * 2 + ox], at_z(zz))

    def slab(p):
        return pl.ds(p * fine, fine)

    def dn_x(zz, p):
        send(r.dn_s.at[zz * 2 + ox, slab(p)], r.dn_r.at[zz, slab(p)],
             r.s_dx.at[zz, p], r.r_dx.at[zz, p], at_x)

    def dn_own(p):
        for zz in (same, across):
            send(r.dn_s.at[zz * 2 + x, slab(p)], at_piece(r.dn_o, f, p),
                 r.s_dl.at[0, zz, p], r.r_dl.at[f, p], at_z(zz))

    def dn_relay(p):
        for zz in (same, across):
            got = r.dn_r.at[zz, slab(p)]
            arrived(got, r.s_dx.at[zz, p], r.r_dx.at[zz, p], at_x)
            send(got, at_piece(r.dn_o, z * 2 + ox, p),
                 r.s_dl.at[1, zz, p], r.r_dl.at[z * 2 + ox, p], at_z(zz))

    own = r.xg.at[t, z, x]
    send(own, own, r.s_tz.at[0], r.r_tz.at[z], at_z(inner))
    send(own, own, r.s_tz.at[1], r.r_tz.at[z], at_z(pair))
    token_x(z)
    up_own(pair)
    for zz in (same, across):
        up_x(zz)
    for zz in (same, across):
        up_own(zz)
    with mark("castdn"):
        fetch[2].wait()
        cast(r.dnm, r.dn_s, r.dn_o, None)
    passed = [
        prepare(r.xg.at[t, zz, x], r.xg.at[t, zz, x], r.s_tz.at[2 + n], r.r_tz.at[zz], at_z(pair), central)
        for n, zz in enumerate((same, across))]

    def token_in(zz):
        token_x(zz)
        token_y(zz, x)
        token_c(y, zz, x)

    with mark("tokpair"):
        arrived(r.xg.at[t, pair, x], r.s_tz.at[0], r.r_tz.at[pair], at_z(pair))
        token_in(pair)
    with mark("toktx0"):
        arrived(r.xg.at[t, z, ox], r.s_tx.at[z], r.r_tx.at[z], at_x)
        token_y(z, ox)
        token_c(y, z, ox)
    up_x(pair)

    def far_tokens():
        for n, zz in enumerate((same, across)):
            arrived(r.xg.at[t, zz, x], r.s_tz.at[0], r.r_tz.at[zz], at_z(pair))

    with mark("tokfarc"):
        @pl.when(central)
        def _():
            far_tokens()
            for copy in passed:
                copy.start()

    with mark("uprelay"):
        for zz in (same, across):
            up_relay(zz)
    with mark("tokfare"):
        pl.when(jnp.logical_not(central))(far_tokens)
        for zz in (same, across):
            token_in(zz)
    send(r.up_s.at[z * 2 + ox], at_rows(r.up_o, f), r.s_up.at[z], r.r_up.at[f], at_x)
    send(r.dn_s.at[pair * 2 + ox], r.dn_r.at[pair], r.s_dx.at[pair, 0], r.r_dx.at[pair, 0], at_x)
    send(r.dn_s.at[z * 2 + ox], at_rows(r.dn_o, f), r.s_de.at[2], r.r_de.at[f], at_x)
    for p in range(PIECES):
        for zz in (same, across):
            dn_x(zz, p)
    with mark("uppair"):
        up_relay(pair)
    send(r.dn_s.at[pair * 2 + x], at_rows(r.dn_o, f), r.s_de.at[0], r.r_de.at[f], at_z(pair))
    for zz in (pair, same, across):
        with mark("toktx"):
            arrived(r.xg.at[t, zz, ox], r.s_tx.at[zz], r.r_tx.at[zz], at_x)
            token_y(zz, ox)
            token_c(y, zz, ox)
    dn_own(0)
    other = oy * 2 + c
    blocks = ((pair, x), (z, ox), (same, x), (across, x), (pair, ox), (same, ox), (across, ox))
    for zz, xx in blocks:
        with mark("tokty"):
            arrived(r.xg.at[other, zz, xx], r.s_ty.at[zz, xx], r.r_ty.at[zz, xx], at_y)
            token_c(oy, zz, xx)
    with mark("dnpair"):
        arrived(r.dn_r.at[pair], r.s_dx.at[pair, 0], r.r_dx.at[pair, 0], at_x)
        send(r.dn_r.at[pair], at_rows(r.dn_o, z * 2 + ox), r.s_de.at[1], r.r_de.at[z * 2 + ox], at_z(pair))
    with mark("dnrel0"):
        dn_relay(0)
    with mark("toktc"):
        for yy in (y, oy):
            for zz, xx in blocks:
                part = r.xg.at[yy * 2 + oc, zz, xx]
                arrived(part, r.s_tc.at[yy, zz, xx], r.r_tc.at[yy, zz, xx], at_c)

    def wait_up(zz, xx):
        k = zz * 2 + xx
        arrived(at_rows(r.up_o, k), r.s_up.at[z], r.r_up.at[k], at_x)

    def up_dot(q, zz):
        return jnp.dot(r.xg[q, zz].reshape(span, cols),
                       r.up_o[pl.ds(pl.multiple_of(q * cols, cols), cols), :],
                       preferred_element_type=F32)

    def at_span(zz):
        return pl.ds(pl.multiple_of(zz * span, span), span)

    with mark("upnear"):
        wait_up(z, ox)
        wait_up(pair, x)
        wait_up(pair, ox)
    with mark("mmnear"):
        @pl.loop(0, nz)
        def _(zz):
            r.pre[at_span(zz), :] = up_dot(close * 2, zz) + up_dot(close * 2 + 1, zz)
    with mark("dnfar1"):
        dn_own(1)
        dn_relay(1)
    with mark("upfar"):
        for zz in (same, across):
            for xx in (x, ox):
                wait_up(zz, xx)
    with mark("mmfar"):
        @pl.loop(0, nz)
        def _(zz):
            low = (1 - close) * 2
            total = r.pre[at_span(zz), :] + up_dot(low, zz) + up_dot(low + 1, zz)
            r.act[at_span(zz), :] = jnp.square(jnp.maximum(total, 0.0)).astype(BF16)
    keep_up = pltpu.make_async_copy(r.up_o, up_h, r.s_out.at[0])
    keep_up.start()

    mine = (y == close, y != close)
    not_mine = (mine[1], mine[0])
    at_pair, at_same = at_z(pair), at_z(same)

    def block_of(u):
        q, part = UNITS[u]
        if part == "far":
            return q, 2 * (1 - close), 2
        if part == "near":
            return q, 2 * close, 2
        return q, 0, nz

    def product(u):
        q, base, n = block_of(u)
        yy, p = (close if q < PIECES else 1 - close), q % PIECES
        if q == 0:
            for zz, xx in ((z, ox), (pair, x), (pair, ox)):
                k = zz * 2 + xx
                arrived(at_rows(r.dn_o, k), r.s_de.at[0], r.r_de.at[k], at_x)
        elif q >= PIECES and UNITS[u][1] != "near":
            for zz in (same, across):
                for xx in (x, ox):
                    k = zz * 2 + xx
                    arrived(at_piece(r.dn_o, k, p), r.s_dl.at[0, zz, p], r.r_dl.at[k, p], at_x)
        taken = jnp.concatenate(
            [at_piece(r.dn_o, yy * 4 + cc * 2 + xx, p)[...] for cc in (oc, c) for xx in range(2)], axis=0)
        total = lax.dot_general(
            r.act[pl.ds(pl.multiple_of(base * span, span), n * span), :], taken,
            (((1,), (1,)), ((), ())), preferred_element_type=F32)
        at = pl.ds(base, n)
        r.cs[q, at] = total[:, :wide].astype(BF16).reshape(n, 2, rows, wide)
        r.part[q, at] = total[:, wide:].reshape(n, 2, rows, wide)
        send(r.cs.at[q, at], r.cr.at[q, at], r.s_c.at[u], r.r_c.at[u], at_c)

    def over(base, n, body):
        @pl.loop(0, n)
        def _(i):
            body(base + i)

    def core_sum(u):
        q, base, n = block_of(u)
        at = pl.ds(base, n)
        arrived(r.cr.at[q, at], r.s_c.at[u], r.r_c.at[u], at_c)
        if q not in Y_FIRST:
            def body(zz):
                r.xb[q, zz] = (r.part[q, zz, ox] + r.cr[q, zz, ox].astype(F32)).astype(BF16)
                r.xs[q, zz] = r.part[q, zz, x] + r.cr[q, zz, x].astype(F32)

            over(base, n, body)
            send(r.xb.at[q, at], r.xr.at[q, at], r.s_x.at[u], r.r_x.at[u], at_x)
        else:
            theirs = not_mine[q // PIECES]
            over_y = prepare(r.fb.at[q, at], r.fr.at[q, at], r.s_y.at[u], r.r_y.at[u], at_y, theirs)

            @pl.when(theirs)
            def _():
                def body(zz):
                    r.fb[q, zz] = (r.part[q, zz] + r.cr[q, zz].astype(F32)).astype(BF16)

                over(base, n, body)
                over_y.start()

    def first_sum(u):
        q, base, n = block_of(u)
        at = pl.ds(base, n)
        if q not in Y_FIRST:
            theirs = not_mine[q // PIECES]
            arrived(r.xr.at[q, at], r.s_x.at[u], r.r_x.at[u], at_x)
            over_y = prepare(r.yb.at[q, at], r.yr.at[q, at], r.s_y.at[u], r.r_y.at[u], at_y, theirs)

            @pl.when(theirs)
            def _():
                def body(zz):
                    r.yb[q, zz] = (r.xs[q, zz] + r.xr[q, zz].astype(F32)).astype(BF16)

                over(base, n, body)
                over_y.start()
        else:
            ours = mine[q // PIECES]
            over_x = prepare(r.xb.at[q, at], r.xr.at[q, at], r.s_x.at[u], r.r_x.at[u], at_x, ours)

            @pl.when(ours)
            def _():
                arrived(r.fr.at[q, at], r.s_y.at[u], r.r_y.at[u], at_y)

                def body(zz):
                    def whole(xx):
                        return (r.part[q, zz, xx] + r.cr[q, zz, xx].astype(F32)
                                + r.fr[q, zz, xx].astype(F32))

                    r.xb[q, zz] = whole(ox).astype(BF16)
                    r.xs[q, zz] = whole(x)

                over(base, n, body)
                over_x.start()

    def second_sum(u):
        q, base, n = block_of(u)
        at, ours, p = pl.ds(base, n), mine[q // PIECES], q % PIECES
        part = UNITS[u][1]
        to_pair = [
            prepare(r.zb.at[p, who], r.zr.at[p, m], r.s_z.at[p, m], r.r_z.at[p, m], at_pair, ours)
            for m, who in ((0, across), (1, pair)) if part != ("near", "far")[m]]

        @pl.when(ours)
        def _():
            if q in Y_FIRST:
                arrived(r.xr.at[q, at], r.s_x.at[u], r.r_x.at[u], at_x)
            else:
                arrived(r.yr.at[q, at], r.s_y.at[u], r.r_y.at[u], at_y)

            def body(zz):
                total = r.xs[q, zz] + r.xr[q, zz].astype(F32)
                if q not in Y_FIRST:
                    total = total + r.yr[q, zz].astype(F32)
                r.kept[p, zz] = total
                r.zb[p, zz] = total.astype(BF16)

            over(base, n, body)
            for copy in to_pair:
                copy.start()

    def cross_sum(u):
        q = UNITS[u][0]
        ours, p = mine[q // PIECES], q % PIECES
        over_z = prepare(r.zc.at[p], r.zr.at[p, 2], r.s_z.at[p, 2], r.r_z.at[p, 2], at_same, ours)

        @pl.when(ours)
        def _():
            arrived(r.zr.at[p, 0], r.s_z.at[p, 0], r.r_z.at[p, 0], at_pair)
            r.zc[p] = (r.kept[p, same] + r.zr[p, 0].astype(F32)).astype(BF16)
            over_z.start()

    def more_down(p):
        dn_own(p)
        dn_relay(p)

    stages = dict(a=product, b=core_sum, c=first_sum, d=second_sum, e=cross_sum, D=more_down)
    for step in ORDER:
        with mark("st_" + step):
            stages[step[0]](int(step[1]))
    keep_dn = pltpu.make_async_copy(r.dn_o, dn_h, r.s_out.at[1])
    keep_dn.start()
    for p in range(PIECES):
        with mark("final%d" % p):
            arrived(r.zr.at[p, 1], r.s_z.at[p, 1], r.r_z.at[p, 1], at_pair)
            arrived(r.zr.at[p, 2], r.s_z.at[p, 2], r.r_z.at[p, 2], at_same)
            total = (r.kept[p, z] + r.zr[p, 1].astype(F32) + r.zr[p, 2].astype(F32)).astype(BF16)
            for xx in range(2):
                mix_o[:, xx * feat + p * fine:xx * feat + (p + 1) * fine] = total[:, xx * fine:(xx + 1) * fine]
    with mark("drain"):
        for copy, when in sent:
            if when is None:
                copy.wait_send()
            else:
                pl.when(when)(copy.wait_send)
        keep_up.wait()
        keep_dn.wait()


UNITS = tuple((q, "all") for q in range(7)) + ((7, "far"), (7, "near"))
Y_FIRST = (0, 4)
ORDER = (
    "a0", "a1", "b0", "a2", "b1", "a3", "b2", "b3", "D2", "a4", "b4", "D3", "c1", "c2", "c0", "a5", "b5",
    "c3", "d1", "c4", "d2", "d0", "a6", "b6", "c5", "d3", "d4", "a7", "a8", "b7", "b8", "c6", "e1", "e2", "e0", "e3",
    "d5", "e4", "c7", "c8", "d6", "e5", "d7", "e6", "d8", "e7",
)


def on_device_fused(tokens, gain, up_master, down_master):
    rows, width = tokens.shape
    feat, ff = up_master.shape
    units = ff // SUB
    nz = SUB // 2
    cols = width // nz
    fine = feat // PIECES
    wide = 2 * fine
    n, pieces = len(UNITS), 2 * PIECES
    dma = pltpu.SemaphoreType.DMA
    vmem = pl.BlockSpec(memory_space=pltpu.VMEM)
    anywhere = pl.BlockSpec(memory_space=pl.ANY)
    arrays = dict(
        tok=((rows, width), BF16), upm=((feat, ff), F32), dnm=((feat, ff), F32),
        up_o=((SUB * feat, units), BF16), dn_o=((SUB * feat, units), BF16),
        xg=((nz, nz, 2, rows, cols), BF16),
        up_s=((SUB, feat, units), BF16), dn_s=((SUB, feat, units), BF16),
        up_r=((nz, feat, units), BF16), dn_r=((nz, feat, units), BF16),
        pre=((SUB * rows, units), F32), act=((SUB * rows, units), BF16),
        cs=((pieces, nz, 2, rows, wide), BF16), cr=((pieces, nz, 2, rows, wide), BF16),
        part=((pieces, nz, 2, rows, wide), F32),
        xs=((pieces, nz, rows, wide), F32), xb=((pieces, nz, rows, wide), BF16), xr=((pieces, nz, rows, wide), BF16),
        yb=((pieces, nz, rows, wide), BF16), yr=((pieces, nz, rows, wide), BF16),
        fb=((pieces, nz, 2, rows, wide), BF16), fr=((pieces, nz, 2, rows, wide), BF16),
        kept=((PIECES, nz, rows, wide), F32), zb=((PIECES, nz, rows, wide), BF16),
        zc=((PIECES, rows, wide), BF16), zr=((PIECES, 3, rows, wide), BF16),
    )
    sems = dict(
        s_in=(3,), s_out=(2,), s_tz=(nz,), r_tz=(nz,), s_tx=(nz,), r_tx=(nz,), s_ty=(nz, 2), r_ty=(nz, 2),
        s_tc=(2, nz, 2), r_tc=(2, nz, 2), s_ux=(nz,), r_ux=(nz,), s_up=(nz,), r_up=(SUB,), s_ur=(nz,),
        s_dx=(nz, PIECES), r_dx=(nz, PIECES), s_de=(3,), r_de=(SUB,), s_dl=(2, nz, PIECES), r_dl=(SUB, PIECES),
        s_c=(n,), r_c=(n,), s_x=(n,), r_x=(n,), s_y=(n,), r_y=(n,), s_z=(PIECES, 3), r_z=(PIECES, 3),
    )
    names = list(arrays) + list(sems)
    up_s, dn_s, mixed = pl.pallas_call(
        functools.partial(fused, nz, names),
        out_shape=(
            jax.ShapeDtypeStruct((SUB * feat, units), BF16),
            jax.ShapeDtypeStruct((SUB * feat, units), BF16),
            jax.ShapeDtypeStruct((rows, cols), BF16),
        ),
        in_specs=[anywhere, vmem, anywhere, anywhere],
        out_specs=(anywhere, anywhere, vmem),
        scratch_shapes=[pltpu.VMEM(*spec) for spec in arrays.values()] + [dma(shape) for shape in sems.values()],
        compiler_params=pltpu.CompilerParams(
            collective_id=0, has_side_effects=True, vmem_limit_bytes=60 * 2**20),
    )(tokens, gain[None, :], up_master, down_master)
    return up_s[None], dn_s[None], mixed


def from_partner(block, axis, bit):
    count = lax.axis_size(axis)
    route = []
    for low in range(count):
        high = low | 1 << bit
        if high != low and high < count:
            route += [(low, high), (high, low)]
    return lax.ppermute(block, axis, route)


def on_device(tokens, gain, up_master, down_master):
    fs_count = lax.axis_size("fs")
    feat_rows = up_master.shape[0]
    units = up_master.shape[1] // SUB
    groups_count = fs_count // SUB
    member = lax.axis_index("fs") % SUB
    up_round = (gain[:, None] * up_master).astype(jnp.bfloat16)
    down_round = down_master.astype(jnp.bfloat16)

    def spread(weight):
        blocks = weight.reshape(feat_rows, SUB, units).transpose(1, 0, 2)
        return jnp.broadcast_to(blocks[None], (groups_count, SUB, feat_rows, units)).reshape(
            fs_count, feat_rows, units
        )

    up_sampled, down_sampled = (
        lax.all_to_all(spread(up_round), "fs", split_axis=0, concat_axis=1, tiled=True),
        lax.all_to_all(spread(down_round), "fs", split_axis=0, concat_axis=1, tiled=True),
    )
    levels = SUB.bit_length() - 1
    bit_list = list(range(levels))
    widened = tokens.astype(jnp.float32)
    normed = (
        widened * lax.rsqrt(jnp.mean(widened * widened, axis=1, keepdims=True) + 1e-06)
    ).astype(jnp.bfloat16)
    current = normed[None]
    for bit in bit_list:
        partner = from_partner(current, "fs", bit)
        lower = member >> bit & 1 == 0
        current = jnp.where(lower, jnp.stack([current, partner]), jnp.stack([partner, current]))
    order_now = list(reversed(bit_list))
    wanted = list(range(levels - 1, -1, -1))
    perm_axes = [
        [place for place, value in enumerate(order_now) if value == target][0] for target in wanted
    ]
    current = jnp.transpose(current, perm_axes + [levels, levels + 1, levels + 2])
    gathered = current.reshape(SUB * tokens.shape[0], tokens.shape[1])
    pre_units = jnp.dot(gathered, up_sampled[0], preferred_element_type=jnp.float32)
    act_units = jnp.square(jax.nn.relu(pre_units)).astype(jnp.bfloat16)
    partial_out = lax.dot_general(
        act_units, down_sampled[0], (((1,), (1,)), ((), ())), preferred_element_type=jnp.float32
    )
    running = partial_out.reshape((2,) * levels + (tokens.shape[0], tokens.shape[1]))
    axis_bits = list(range(levels - 1, -1, -1))
    for bit in bit_list:
        position = len([value for value in axis_bits if value > bit])
        mine = member >> bit & 1
        keep = lax.dynamic_index_in_dim(running, mine, position, keepdims=False)
        other = lax.dynamic_index_in_dim(running, 1 - mine, position, keepdims=False)
        running = keep + from_partner(other, "fs", bit)
        axis_bits = [value for value in axis_bits if value != bit]
    summed = lax.psum_scatter(running, "tp", scatter_dimension=1, tiled=True)
    return (up_sampled, down_sampled, summed.astype(jnp.bfloat16))


def solution(mesh):
    placed = (P("fs", None), P("fs"), P("fs", "tp"), P("fs", "tp"))
    one_group = mesh.shape["fs"] == SUB and mesh.shape["tp"] == 4
    return jax.shard_map(
        on_device_fused if one_group else on_device,
        mesh=mesh,
        in_specs=placed,
        out_specs=(P("fs", None, "tp"), P("fs", None, "tp"), P("fs", "tp")),
        check_vma=False,
    )
```

```python
import collections
import functools
import math
import types

import jax
import jax.numpy as jnp
from jax import lax
from jax.experimental import pallas as pl
from jax.experimental.pallas import tpu as pltpu
from jax.sharding import PartitionSpec as P

SUB = 8
EPS = 1e-06
BF16 = jnp.bfloat16
F32 = jnp.float32
PIECES = 4


def fused(nz, names, tok_h, gain, upm_h, dnm_h, up_o, dn_o, mix_o, *refs):
    r = types.SimpleNamespace(**dict(zip(names, refs)))
    r.up_o, r.dn_o = up_o, dn_o
    mark = jax.named_scope
    f, t = lax.axis_index("fs"), lax.axis_index("tp")
    z, x = f // 2, f % 2
    y, c = t // 2, t % 2
    ox, oy, oc = 1 - x, 1 - y, 1 - c
    rows, width = r.tok.shape
    cols = width // nz
    feat = r.upm.shape[0]
    units = r.act.shape[1]
    fine = feat // PIECES
    wide = 2 * fine
    span = 2 * rows
    close = z // 2
    same = (z + 2) % 4
    pair = z + 1 - 2 * (z % 2)
    across = (pair + 2) % 4
    inner, outer = 2 - close, 3 * (1 - close)
    central = jnp.logical_or(z == 1, z == 2)
    at_x = (z * 2 + ox, t)
    at_y = (f, oy * 2 + c)
    at_c = (f, y * 2 + oc)

    def at_z(zz):
        return (zz * 2 + x, t)

    fetch = [pltpu.make_async_copy(src, dst, r.s_in.at[n]) for n, (src, dst) in enumerate(
        ((tok_h, r.tok), (upm_h, r.upm), (dnm_h, r.dnm)))]
    for copy in fetch:
        copy.start()

    barrier = pltpu.get_barrier_semaphore()
    partners = (at_z(pair), at_z(same), at_z(across), at_x, at_y, at_c)
    for dev in partners:
        pl.semaphore_signal(barrier, inc=1, device_id=dev, device_id_type=pl.DeviceIdType.MESH)

    tally = collections.Counter()

    def remote(src, dst, kind, rsem, dev, counted=True):
        if counted:
            tally[kind] += math.prod(src.shape) * jnp.dtype(src.dtype).itemsize
        return pltpu.make_async_remote_copy(
            src_ref=src, dst_ref=dst, send_sem=r.s_out.at[kind], recv_sem=rsem,
            device_id=dev, device_id_type=pl.DeviceIdType.MESH)

    def send(src, dst, kind, rsem, dev):
        remote(src, dst, kind, rsem, dev).start()

    def arrived(dst, rsem):
        remote(dst, dst, 0, rsem, at_x, False).wait_recv()

    def slot(q, zz, xx):
        return (q * nz + zz) * 2 + xx

    def token(q, zz, xx):
        return r.xg.at[slot(q, zz, xx)]

    def blocks_of(n):
        return r.xg.at[pl.ds(0, n)]

    def at_rows(ref, k):
        return ref.at[pl.ds(pl.multiple_of(k * feat, feat), feat), :]

    def at_piece(ref, k, p):
        return ref.at[pl.ds(pl.multiple_of(k * feat + p * fine, fine), fine), :]

    def cast(src, dst, out, factor):
        for m in range(SUB):
            block = src[:, m * units:(m + 1) * units]
            dst[m] = (block if factor is None else factor * block).astype(BF16)
        block = src[:, pl.ds(pl.multiple_of(f * units, units), units)]
        out[pl.ds(pl.multiple_of(f * feat, feat), feat), :] = (
            block if factor is None else factor * block).astype(BF16)

    with mark("norm"):
        fetch[0].wait()
        full = r.tok[...].astype(F32)
        scale = lax.rsqrt(jnp.mean(full * full, axis=1, keepdims=True) + EPS)
        for q in range(nz):
            r.xg[slot(q, z, x)] = (full[:, q * cols:(q + 1) * cols] * scale).astype(BF16)
    with mark("barrier"):
        pl.semaphore_wait(barrier, len(partners))

    TOKEN, WEIGHT, SUM, PASSED = range(4)

    def token_x(zz):
        send(token(t, zz, x), token(t, zz, x), TOKEN, r.r_tx.at[zz], at_x)

    def token_y(zz, xx):
        send(token(t, zz, xx), token(t, zz, xx), TOKEN, r.r_ty.at[zz, xx], at_y)

    def token_c(yy, zz, xx):
        part = token(yy * 2 + c, zz, xx)
        send(part, part, TOKEN, r.r_tc.at[0], at_c)

    def token_in(zz):
        token_x(zz)
        token_y(zz, x)
        token_c(y, zz, x)

    def up_x(zz):
        send(r.up_s.at[zz * 2 + ox], r.up_r.at[zz], WEIGHT, r.r_ux.at[zz], at_x)

    def up_own(zz, far):
        send(r.up_s.at[zz * 2 + x], at_rows(r.up_o, f), WEIGHT, r.r_up.at[far], at_z(zz))

    def up_relay(zz, far):
        arrived(r.up_r.at[zz], r.r_ux.at[zz])
        send(r.up_r.at[zz], at_rows(r.up_o, z * 2 + ox), WEIGHT, r.r_up.at[far], at_z(zz))

    def slab(p):
        return pl.ds(p * fine, fine)

    def dn_x(p):
        for zz in (inner, outer):
            send(r.dn_s.at[zz * 2 + ox, slab(p)], r.dn_r.at[zz, slab(p)], WEIGHT, r.r_dx.at[p], at_x)

    def dn_own(p):
        for zz in (inner, outer):
            send(r.dn_s.at[zz * 2 + x, slab(p)], at_piece(r.dn_o, f, p), WEIGHT, r.r_dl.at[p], at_z(zz))

    def dn_relay(p):
        arrived(r.dn_r.at[pl.ds(0, 2), slab(p)], r.r_dx.at[p])
        for zz in (inner, outer):
            send(r.dn_r.at[zz, slab(p)], at_piece(r.dn_o, z * 2 + ox, p), WEIGHT, r.r_dl.at[p], at_z(zz))

    for to in (inner, pair):
        send(token(t, z, x), token(t, z, x), TOKEN, r.r_tz.at[z], at_z(to))
    token_x(z)
    with mark("castup"):
        fetch[1].wait()
        cast(r.upm, r.up_s, r.up_o, jnp.transpose(gain[...]))
    up_own(pair, 0)
    for zz in (inner, outer):
        up_x(zz)
    for zz in (inner, outer):
        up_own(zz, 1)
    with mark("castdn"):
        fetch[2].wait()
        cast(r.dnm, r.dn_s, r.dn_o, None)
    passed = [
        remote(token(t, zz, x), token(t, zz, x), PASSED, r.r_tz.at[zz], at_z(pair)) for zz in (inner, outer)]
    with mark("tokpair"):
        arrived(token(t, pair, x), r.r_tz.at[pair])
        token_in(pair)
    with mark("toktx0"):
        arrived(token(t, z, ox), r.r_tx.at[z])
        token_y(z, ox)
        token_c(y, z, ox)
    up_x(pair)

    def far_tokens():
        for zz in (inner, outer):
            arrived(token(t, zz, x), r.r_tz.at[zz])

    with mark("tokfarc"):
        @pl.when(central)
        def _():
            far_tokens()
            for copy in passed:
                copy.start()

    with mark("uprelay"):
        for zz in (inner, outer):
            up_relay(zz, 1)
    with mark("tokfare"):
        pl.when(jnp.logical_not(central))(far_tokens)
        for zz in (inner, outer):
            token_in(zz)
    send(r.up_s.at[z * 2 + ox], at_rows(r.up_o, f), WEIGHT, r.r_up.at[0], at_x)
    send(r.dn_s.at[pair * 2 + ox], r.dn_r.at[pair], WEIGHT, r.r_dx.at[PIECES], at_x)
    send(r.dn_s.at[z * 2 + ox], at_rows(r.dn_o, f), WEIGHT, r.r_de.at[0], at_x)
    for p in range(PIECES):
        dn_x(p)
    with mark("uppair"):
        up_relay(pair, 0)
    send(r.dn_s.at[pair * 2 + x], at_rows(r.dn_o, f), WEIGHT, r.r_de.at[0], at_z(pair))
    for zz in (pair, inner, outer):
        with mark("toktx"):
            arrived(token(t, zz, ox), r.r_tx.at[zz])
            token_y(zz, ox)
            token_c(y, zz, ox)
    dn_own(0)
    other = oy * 2 + c
    for zz, xx in ((pair, x), (z, ox), (inner, x), (outer, x), (pair, ox), (inner, ox), (outer, ox)):
        with mark("tokty"):
            arrived(token(other, zz, xx), r.r_ty.at[zz, xx])
            token_c(oy, zz, xx)
    with mark("dnpair"):
        arrived(r.dn_r.at[pair], r.r_dx.at[PIECES])
        send(r.dn_r.at[pair], at_rows(r.dn_o, z * 2 + ox), WEIGHT, r.r_de.at[0], at_z(pair))
    with mark("dnrel0"):
        dn_relay(0)
    with mark("toktc"):
        arrived(blocks_of(2 * (2 * nz - 1)), r.r_tc.at[0])

    def up_dot(q, zz):
        return jnp.dot(r.xg[pl.ds(slot(q, zz, 0), 2)].reshape(span, cols),
                       r.up_o[pl.ds(pl.multiple_of(q * cols, cols), cols), :],
                       preferred_element_type=F32)

    def at_span(zz):
        return pl.ds(pl.multiple_of(zz * span, span), span)

    with mark("upnear"):
        arrived(blocks_of(3), r.r_up.at[0])
    with mark("mmnear"):
        @pl.loop(0, nz)
        def _(zz):
            r.pre[at_span(zz), :] = up_dot(close * 2, zz) + up_dot(close * 2 + 1, zz)
    with mark("dnfar1"):
        dn_own(1)
        dn_relay(1)
    with mark("upfar"):
        arrived(blocks_of(4), r.r_up.at[1])
    with mark("mmfar"):
        @pl.loop(0, nz)
        def _(zz):
            low = (1 - close) * 2
            total = r.pre[at_span(zz), :] + up_dot(low, zz) + up_dot(low + 1, zz)
            r.act[at_span(zz), :] = jnp.square(jnp.maximum(total, 0.0)).astype(BF16)

    mine = (y == close, y != close)
    not_mine = (mine[1], mine[0])
    at_pair, at_same = at_z(pair), at_z(same)

    def block_of(u):
        q, part = UNITS[u]
        if part == "far":
            return q, 2 * (1 - close), 2
        if part == "near":
            return q, 2 * close, 2
        return q, 0, nz

    def product(u):
        q, base, n = block_of(u)
        yy, p = (close if q < PIECES else 1 - close), q % PIECES
        if q == 0:
            arrived(blocks_of(3), r.r_de.at[0])
        elif q >= PIECES and UNITS[u][1] != "near":
            arrived(blocks_of(1), r.r_dl.at[p])
        taken = jnp.concatenate(
            [at_piece(r.dn_o, yy * 4 + cc * 2 + xx, p)[...] for cc in (oc, c) for xx in range(2)], axis=0)
        total = lax.dot_general(
            r.act[pl.ds(pl.multiple_of(base * span, span), n * span), :], taken,
            (((1,), (1,)), ((), ())), preferred_element_type=F32)
        at = pl.ds(base, n)
        r.cs[q, at] = total[:, :wide].astype(BF16).reshape(n, 2, rows, wide)
        r.part[q, at] = total[:, wide:].reshape(n, 2, rows, wide)
        send(r.cs.at[q, at], r.cr.at[q, at], SUM, r.r_c.at[u], at_c)

    def over(base, n, body):
        @pl.loop(0, n)
        def _(i):
            body(base + i)

    def core_sum(u):
        q, base, n = block_of(u)
        at = pl.ds(base, n)
        arrived(r.cr.at[q, at], r.r_c.at[u])
        if q not in Y_FIRST:
            def body(zz):
                r.xb[q, zz] = (r.part[q, zz, ox] + r.cr[q, zz, ox].astype(F32)).astype(BF16)
                r.xs[q, zz] = r.part[q, zz, x] + r.cr[q, zz, x].astype(F32)

            over(base, n, body)
            send(r.xb.at[q, at], r.xr.at[q, at], SUM, r.r_x.at[u], at_x)
        else:
            theirs = not_mine[q // PIECES]
            over_y = remote(r.fb.at[q, at], r.fr.at[q, at], SUM, r.r_y.at[u], at_y, q < PIECES)

            @pl.when(theirs)
            def _():
                def body(zz):
                    r.fb[q, zz] = (r.part[q, zz] + r.cr[q, zz].astype(F32)).astype(BF16)

                over(base, n, body)
                over_y.start()

    def first_sum(u):
        q, base, n = block_of(u)
        at = pl.ds(base, n)
        if q not in Y_FIRST:
            theirs = not_mine[q // PIECES]
            arrived(r.xr.at[q, at], r.r_x.at[u])
            over_y = remote(r.yb.at[q, at], r.yr.at[q, at], SUM, r.r_y.at[u], at_y, q < PIECES)

            @pl.when(theirs)
            def _():
                def body(zz):
                    r.yb[q, zz] = (r.xs[q, zz] + r.xr[q, zz].astype(F32)).astype(BF16)

                over(base, n, body)
                over_y.start()
        else:
            ours = mine[q // PIECES]
            over_x = remote(r.xb.at[q, at], r.xr.at[q, at], SUM, r.r_x.at[u], at_x, q < PIECES)

            @pl.when(ours)
            def _():
                arrived(r.fr.at[q, at], r.r_y.at[u])

                def body(zz):
                    def whole(xx):
                        return (r.part[q, zz, xx] + r.cr[q, zz, xx].astype(F32)
                                + r.fr[q, zz, xx].astype(F32))

                    r.xb[q, zz] = whole(ox).astype(BF16)
                    r.xs[q, zz] = whole(x)

                over(base, n, body)
                over_x.start()

    def second_sum(u):
        q, base, n = block_of(u)
        at, ours, p = pl.ds(base, n), mine[q // PIECES], q % PIECES
        part = UNITS[u][1]
        to_pair = [
            remote(r.zb.at[p, who], r.zr.at[p, m], SUM, r.r_z.at[p, m], at_pair, q < PIECES)
            for m, who in ((0, across), (1, pair)) if part != ("near", "far")[m]]

        @pl.when(ours)
        def _():
            if q in Y_FIRST:
                arrived(r.xr.at[q, at], r.r_x.at[u])
            else:
                arrived(r.yr.at[q, at], r.r_y.at[u])

            def body(zz):
                total = r.xs[q, zz] + r.xr[q, zz].astype(F32)
                if q not in Y_FIRST:
                    total = total + r.yr[q, zz].astype(F32)
                r.kept[p, zz] = total
                r.zb[p, zz] = total.astype(BF16)

            over(base, n, body)
            for copy in to_pair:
                copy.start()

    def cross_sum(u):
        q = UNITS[u][0]
        ours, p = mine[q // PIECES], q % PIECES
        over_z = remote(r.zc.at[p], r.zr.at[p, 2], SUM, r.r_z.at[p, 1], at_same, q < PIECES)

        @pl.when(ours)
        def _():
            arrived(r.zr.at[p, 0], r.r_z.at[p, 0])
            r.zc[p] = (r.kept[p, same] + r.zr[p, 0].astype(F32)).astype(BF16)
            over_z.start()

    def more_down(p):
        dn_own(p)
        dn_relay(p)

    stages = dict(a=product, b=core_sum, c=first_sum, d=second_sum, e=cross_sum, D=more_down)
    for step in ORDER:
        with mark("st_" + step):
            stages[step[0]](int(step[1]))
    for p in range(PIECES):
        with mark("final%d" % p):
            arrived(r.zr.at[p, pl.ds(1, 2)], r.r_z.at[p, 1])
            total = (r.kept[p, z] + r.zr[p, 1].astype(F32) + r.zr[p, 2].astype(F32)).astype(BF16)
            for xx in range(2):
                mix_o[:, xx * feat + p * fine:xx * feat + (p + 1) * fine] = total[:, xx * fine:(xx + 1) * fine]
    with mark("drain"):
        block = rows * cols * jnp.dtype(BF16).itemsize

        def wait_sent(kind):
            assert tally[kind] % block == 0
            done = blocks_of(tally[kind] // block)
            remote(done, done, kind, r.r_tc.at[0], at_x, False).wait_send()

        for kind in (TOKEN, WEIGHT, SUM):
            wait_sent(kind)
        pl.when(central)(lambda: wait_sent(PASSED))


UNITS = tuple((q, "all") for q in range(7)) + ((7, "far"), (7, "near"))
Y_FIRST = (0, 4)
ORDER = (
    "a0", "a1", "b0", "a2", "b1", "a3", "b2", "b3", "D2", "a4", "b4", "D3", "c1", "c2", "c0", "a5", "b5",
    "c3", "d1", "c4", "d2", "d0", "a6", "b6", "c5", "d3", "d4", "a7", "a8", "b7", "b8", "c6", "e1", "e2", "e0", "e3",
    "d5", "e4", "c7", "c8", "d6", "e5", "d7", "e6", "d8", "e7",
)


def on_device_fused(tokens, gain, up_master, down_master):
    rows, width = tokens.shape
    feat, ff = up_master.shape
    units = ff // SUB
    nz = SUB // 2
    cols = width // nz
    fine = feat // PIECES
    wide = 2 * fine
    n, pieces = len(UNITS), 2 * PIECES
    dma = pltpu.SemaphoreType.DMA
    vmem = pl.BlockSpec(memory_space=pltpu.VMEM)
    hbm = pl.BlockSpec(memory_space=pltpu.HBM)
    anywhere = pl.BlockSpec(memory_space=pl.ANY)
    arrays = dict(
        tok=((rows, width), BF16), upm=((feat, ff), F32), dnm=((feat, ff), F32),
        xg=((2 * nz * nz, rows, cols), BF16),
        up_s=((SUB, feat, units), BF16), dn_s=((SUB, feat, units), BF16),
        up_r=((nz, feat, units), BF16), dn_r=((nz, feat, units), BF16),
        pre=((SUB * rows, units), F32), act=((SUB * rows, units), BF16),
        cs=((pieces, nz, 2, rows, wide), BF16), cr=((pieces, nz, 2, rows, wide), BF16),
        part=((pieces, nz, 2, rows, wide), F32),
        xs=((pieces, nz, rows, wide), F32), xb=((pieces, nz, rows, wide), BF16), xr=((pieces, nz, rows, wide), BF16),
        yb=((pieces, nz, rows, wide), BF16), yr=((pieces, nz, rows, wide), BF16),
        fb=((pieces, nz, 2, rows, wide), BF16), fr=((pieces, nz, 2, rows, wide), BF16),
        kept=((PIECES, nz, rows, wide), F32), zb=((PIECES, nz, rows, wide), BF16),
        zc=((PIECES, rows, wide), BF16), zr=((PIECES, 3, rows, wide), BF16),
    )
    sems = dict(
        s_in=(3,), s_out=(4,), r_tz=(nz,), r_tx=(nz,), r_ty=(nz, 2), r_tc=(1,), r_ux=(nz,), r_up=(2,),
        r_dx=(PIECES + 1,), r_de=(1,), r_dl=(PIECES,), r_c=(n,), r_x=(n,), r_y=(n,), r_z=(PIECES, 2),
    )
    names = list(arrays) + list(sems)
    up_s, dn_s, mixed = pl.pallas_call(
        functools.partial(fused, nz, names),
        out_shape=(
            pltpu.VMEM((SUB * feat, units), BF16),
            pltpu.VMEM((SUB * feat, units), BF16),
            pltpu.VMEM((rows, cols), BF16),
        ),
        in_specs=[hbm, vmem, hbm, hbm],
        out_specs=(vmem, vmem, vmem),
        scratch_shapes=[pltpu.VMEM(*spec) for spec in arrays.values()] + [dma(shape) for shape in sems.values()],
        compiler_params=pltpu.CompilerParams(
            collective_id=0, has_side_effects=True, vmem_limit_bytes=62873 * 2**10),
    )(tokens, gain[None, :], up_master, down_master)
    shapes = [jax.ShapeDtypeStruct(a.shape, a.dtype) for a in (up_s, dn_s, mixed)]
    up_s, dn_s, mixed = pl.pallas_call(
        write_out, out_shape=shapes, in_specs=[anywhere] * 3, out_specs=[anywhere] * 3,
        scratch_shapes=[dma((3,))],
        compiler_params=pltpu.CompilerParams(vmem_limit_bytes=2**20),
    )(up_s, dn_s, mixed)
    return up_s[None], dn_s[None], mixed


def write_out(*refs):
    copies = [pltpu.make_async_copy(refs[n], refs[3 + n], refs[6].at[n]) for n in range(3)]
    for copy in copies:
        copy.start()
    for copy in copies:
        copy.wait()


def from_partner(block, axis, bit):
    count = lax.axis_size(axis)
    route = []
    for low in range(count):
        high = low | 1 << bit
        if high != low and high < count:
            route += [(low, high), (high, low)]
    return lax.ppermute(block, axis, route)


def on_device(tokens, gain, up_master, down_master):
    fs_count = lax.axis_size("fs")
    feat_rows = up_master.shape[0]
    units = up_master.shape[1] // SUB
    groups_count = fs_count // SUB
    member = lax.axis_index("fs") % SUB
    up_round = (gain[:, None] * up_master).astype(jnp.bfloat16)
    down_round = down_master.astype(jnp.bfloat16)

    def spread(weight):
        blocks = weight.reshape(feat_rows, SUB, units).transpose(1, 0, 2)
        return jnp.broadcast_to(blocks[None], (groups_count, SUB, feat_rows, units)).reshape(
            fs_count, feat_rows, units
        )

    up_sampled, down_sampled = (
        lax.all_to_all(spread(up_round), "fs", split_axis=0, concat_axis=1, tiled=True),
        lax.all_to_all(spread(down_round), "fs", split_axis=0, concat_axis=1, tiled=True),
    )
    levels = SUB.bit_length() - 1
    bit_list = list(range(levels))
    widened = tokens.astype(jnp.float32)
    normed = (
        widened * lax.rsqrt(jnp.mean(widened * widened, axis=1, keepdims=True) + 1e-06)
    ).astype(jnp.bfloat16)
    current = normed[None]
    for bit in bit_list:
        partner = from_partner(current, "fs", bit)
        lower = member >> bit & 1 == 0
        current = jnp.where(lower, jnp.stack([current, partner]), jnp.stack([partner, current]))
    order_now = list(reversed(bit_list))
    wanted = list(range(levels - 1, -1, -1))
    perm_axes = [
        [place for place, value in enumerate(order_now) if value == target][0] for target in wanted
    ]
    current = jnp.transpose(current, perm_axes + [levels, levels + 1, levels + 2])
    gathered = current.reshape(SUB * tokens.shape[0], tokens.shape[1])
    pre_units = jnp.dot(gathered, up_sampled[0], preferred_element_type=jnp.float32)
    act_units = jnp.square(jax.nn.relu(pre_units)).astype(jnp.bfloat16)
    partial_out = lax.dot_general(
        act_units, down_sampled[0], (((1,), (1,)), ((), ())), preferred_element_type=jnp.float32
    )
    running = partial_out.reshape((2,) * levels + (tokens.shape[0], tokens.shape[1]))
    axis_bits = list(range(levels - 1, -1, -1))
    for bit in bit_list:
        position = len([value for value in axis_bits if value > bit])
        mine = member >> bit & 1
        keep = lax.dynamic_index_in_dim(running, mine, position, keepdims=False)
        other = lax.dynamic_index_in_dim(running, 1 - mine, position, keepdims=False)
        running = keep + from_partner(other, "fs", bit)
        axis_bits = [value for value in axis_bits if value != bit]
    summed = lax.psum_scatter(running, "tp", scatter_dimension=1, tiled=True)
    return (up_sampled, down_sampled, summed.astype(jnp.bfloat16))


def solution(mesh):
    placed = (P("fs", None), P("fs"), P("fs", "tp"), P("fs", "tp"))
    one_group = mesh.shape["fs"] == SUB and mesh.shape["tp"] == 4
    return jax.shard_map(
        on_device_fused if one_group else on_device,
        mesh=mesh,
        in_specs=placed,
        out_specs=(P("fs", None, "tp"), P("fs", None, "tp"), P("fs", "tp")),
        check_vma=False,
    )
```

```python
import collections
import functools
import math
import types

import jax
import jax.numpy as jnp
from jax import lax
from jax.experimental import pallas as pl
from jax.experimental.pallas import tpu as pltpu
from jax.sharding import PartitionSpec as P

SUB = 8
EPS = 1e-06
BF16 = jnp.bfloat16
F32 = jnp.float32
PIECES = 4


def fused(nz, names, tok_h, gain, upm_h, dnm_h, up_o, dn_o, mix_o, *refs):
    r = types.SimpleNamespace(**dict(zip(names, refs)))
    r.up_o, r.dn_o = up_o, dn_o
    mark = jax.named_scope
    f, t = lax.axis_index("fs"), lax.axis_index("tp")
    z, x = f // 2, f % 2
    y, c = t // 2, t % 2
    ox, oy, oc = 1 - x, 1 - y, 1 - c
    rows, width = r.tok.shape
    cols = width // nz
    feat = r.upm.shape[0]
    units = r.act.shape[1]
    fine = feat // PIECES
    wide, half_wide = 4 * fine, 2 * fine
    span = 2 * rows
    close = z // 2
    same = (z + 2) % 4
    pair = z + 1 - 2 * (z % 2)
    across = (pair + 2) % 4
    inner, outer = 2 - close, 3 * (1 - close)
    central = jnp.logical_or(z == 1, z == 2)
    at_x = (z * 2 + ox, t)
    at_y = (f, oy * 2 + c)
    at_c = (f, y * 2 + oc)

    def at_z(zz):
        return (zz * 2 + x, t)

    fetch = [pltpu.make_async_copy(src, dst, r.s_in.at[n]) for n, (src, dst) in enumerate(
        ((tok_h, r.tok), (upm_h, r.upm), (dnm_h, r.dnm)))]
    for copy in fetch:
        copy.start()

    barrier = pltpu.get_barrier_semaphore()
    def greet(dev):
        pl.semaphore_signal(barrier, inc=1, device_id=dev, device_id_type=pl.DeviceIdType.MESH)

    for dev in (at_z(pair), at_x, at_y, at_c):
        greet(dev)

    @pl.when(central)
    def _():
        greet(at_z(inner))
        greet(at_z(outer))

    tally = collections.Counter()

    def remote(src, dst, kind, rsem, dev, counted=True):
        if counted:
            tally[kind] += math.prod(src.shape) * jnp.dtype(src.dtype).itemsize
        return pltpu.make_async_remote_copy(
            src_ref=src, dst_ref=dst, send_sem=r.s_out.at[kind], recv_sem=rsem,
            device_id=dev, device_id_type=pl.DeviceIdType.MESH)

    def send(src, dst, kind, rsem, dev):
        remote(src, dst, kind, rsem, dev).start()

    def arrived(dst, rsem):
        remote(dst, dst, 0, rsem, at_x, False).wait_recv()

    def slot(q, zz, xx):
        return (q * nz + zz) * 2 + xx

    def token(q, zz, xx):
        return r.xg.at[slot(q, zz, xx)]

    def blocks_of(n):
        return r.xg.at[pl.ds(0, n)]

    def at_rows(ref, k):
        return ref.at[pl.ds(pl.multiple_of(k * feat, feat), feat), :]

    def at_piece(ref, k, p):
        return ref.at[pl.ds(pl.multiple_of(k * feat + p * fine, fine), fine), :]

    def cast(src, dst, out, factor):
        for m in range(SUB):
            block = src[:, m * units:(m + 1) * units]
            dst[m] = (block if factor is None else factor * block).astype(BF16)
        block = src[:, pl.ds(pl.multiple_of(f * units, units), units)]
        out[pl.ds(pl.multiple_of(f * feat, feat), feat), :] = (
            block if factor is None else factor * block).astype(BF16)

    with mark("norm"):
        fetch[0].wait()
        full = r.tok[...].astype(F32)
        scale = lax.rsqrt(jnp.mean(full * full, axis=1, keepdims=True) + EPS)
        for q in range(nz):
            r.xg[slot(q, z, x)] = (full[:, q * cols:(q + 1) * cols] * scale).astype(BF16)
    with mark("barrier"):
        pl.semaphore_wait(barrier, 5)

    TOKEN, WEIGHT, SUM, PASSED, OURS, THEIRS = range(6)

    def hop(q, zz, xx, rsem, dev, kind=TOKEN):
        return remote(token(q, zz, xx), token(q, zz, xx), kind, rsem, dev)

    other = oy * 2 + c
    at = dict(own=z, pair=pair, inner=inner, outer=outer)
    at_xx = dict(x=x, ox=ox)
    over_x = {w: hop(t, zz, x, r.r_tx.at[zz], at_x) for w, zz in at.items()}
    places = [(w, xx) for w in at for xx in at_xx if (w, xx) != ("own", "x")]
    over_y = {(w, xx): hop(t, at[w], at_xx[xx], r.r_ty.at[at[w], at_xx[xx]], at_y) for w, xx in places}
    over_c = {(n, w, xx): hop(q, at[w], at_xx[xx], r.r_tc.at[0], at_c)
              for n, q in enumerate((t, other)) for w, xx in places}
    passed = {w: hop(t, at[w], x, r.r_tz.at[at[w]], at_z(pair), PASSED) for w in ("inner", "outer")}

    def spread(w, xx):
        over_y[w, xx].start()
        over_c[0, w, xx].start()

    def from_z(w, relayed=False):
        arrived(token(t, at[w], x), r.r_tz.at[at[w]])
        if relayed:
            passed[w].start()
        over_x[w].start()
        spread(w, "x")

    def from_x(w):
        arrived(token(t, at[w], ox), r.r_tx.at[at[w]])
        spread(w, "ox")

    def from_y(w, xx):
        arrived(token(other, at[w], at_xx[xx]), r.r_ty.at[at[w], at_xx[xx]])
        over_c[1, w, xx].start()

    def either(when_central, when_end):
        pl.when(central)(when_central)
        pl.when(jnp.logical_not(central))(when_end)

    def up_x(zz):
        send(r.up_s.at[zz * 2 + ox], r.up_r.at[zz], WEIGHT, r.r_ux.at[zz], at_x)

    def up_own(zz, far, counted=True):
        remote(r.up_s.at[zz * 2 + x], at_rows(r.up_o, f), WEIGHT, r.r_up.at[far], at_z(zz), counted).start()

    def up_relay(zz, far):
        arrived(r.up_r.at[zz], r.r_ux.at[zz])
        send(r.up_r.at[zz], at_rows(r.up_o, z * 2 + ox), WEIGHT, r.r_up.at[far], at_z(zz))

    def slab(p):
        return pl.ds(p * fine, fine)

    def dn_x(p):
        for zz in (inner, outer):
            send(r.dn_s.at[zz * 2 + ox, slab(p)], r.dn_r.at[zz, slab(p)], WEIGHT, r.r_dx.at[p], at_x)

    def dn_own(p):
        for zz in (inner, outer):
            send(r.dn_s.at[zz * 2 + x, slab(p)], at_piece(r.dn_o, f, p), WEIGHT, r.r_dl.at[p], at_z(zz))

    def dn_relay(p):
        arrived(r.dn_r.at[pl.ds(0, 2), slab(p)], r.r_dx.at[p])
        for zz in (inner, outer):
            send(r.dn_r.at[zz, slab(p)], at_piece(r.dn_o, z * 2 + ox, p), WEIGHT, r.r_dl.at[p], at_z(zz))

    for to in (inner, pair):
        hop(t, z, x, r.r_tz.at[z], at_z(to)).start()
    over_x["own"].start()
    with mark("castup"):
        fetch[1].wait()
        cast(r.upm, r.up_s, r.up_o, jnp.transpose(gain[...]))
    up_own(pair, 0)
    up_x(pair)
    up_x(inner)
    up_own(inner, 1)
    with mark("castdn"):
        fetch[2].wait()
        cast(r.dnm, r.dn_s, r.dn_o, None)

    def central_first():
        with mark("cinner"):
            from_z("inner", True)
        with mark("couter"):
            from_z("outer", True)

    def end_first():
        with mark("epair"):
            from_z("pair")
        with mark("exz"):
            from_x("own")

    either(central_first, end_first)
    up_x(outer)

    def central_second():
        with mark("cpair"):
            from_z("pair")
        with mark("cxz"):
            from_x("own")

    pl.when(central)(central_second)
    with mark("uppair"):
        up_relay(pair, 0)
    send(r.dn_s.at[pair * 2 + x], at_rows(r.dn_o, f), WEIGHT, r.r_de.at[0], at_z(pair))
    with mark("uprelay"):
        up_relay(inner, 1)

    def central_third():
        up_own(outer, 1)
        with mark("cxinner"):
            from_x("inner")
        with mark("cxouter"):
            from_x("outer")

    def end_third():
        with mark("expair"):
            from_x("pair")
        with mark("einner"):
            from_z("inner")
        with mark("eouter"):
            from_z("outer")
        up_own(outer, 1, False)

    either(central_third, end_third)
    send(r.dn_s.at[pair * 2 + ox], r.dn_r.at[pair], WEIGHT, r.r_dx.at[PIECES], at_x)
    send(r.up_s.at[z * 2 + ox], at_rows(r.up_o, f), WEIGHT, r.r_up.at[0], at_x)
    send(r.dn_s.at[z * 2 + ox], at_rows(r.dn_o, f), WEIGHT, r.r_de.at[0], at_x)
    for p in range(PIECES):
        dn_x(p)
    with mark("uprelay"):
        up_relay(outer, 1)
    dn_own(0)

    def central_fourth():
        with mark("cxpair"):
            from_x("pair")

    def end_fourth():
        with mark("exinner"):
            from_x("inner")
        with mark("exouter"):
            from_x("outer")

    def central_fifth():
        with mark("cy"):
            for w, xx in (("inner", "x"), ("outer", "x"), ("pair", "x"), ("own", "ox"),
                          ("inner", "ox"), ("outer", "ox"), ("pair", "ox")):
                from_y(w, xx)

    def end_fifth():
        with mark("ey"):
            for w, xx in (("pair", "x"), ("own", "ox"), ("pair", "ox"), ("inner", "x"),
                          ("outer", "x"), ("inner", "ox"), ("outer", "ox")):
                from_y(w, xx)

    either(central_fourth, end_fourth)
    with mark("dnpair"):
        arrived(r.dn_r.at[pair], r.r_dx.at[PIECES])
        send(r.dn_r.at[pair], at_rows(r.dn_o, z * 2 + ox), WEIGHT, r.r_de.at[0], at_z(pair))
    either(central_fifth, end_fifth)
    with mark("toktc"):
        arrived(blocks_of(2 * (2 * nz - 1)), r.r_tc.at[0])

    def up_dot(q, zz):
        return jnp.dot(r.xg[pl.ds(slot(q, zz, 0), 2)].reshape(span, cols),
                       r.up_o[pl.ds(pl.multiple_of(q * cols, cols), cols), :],
                       preferred_element_type=F32)

    def at_span(zz):
        return pl.ds(pl.multiple_of(zz * span, span), span)

    with mark("upnear"):
        arrived(blocks_of(3), r.r_up.at[0])
    with mark("mmnear"):
        @pl.loop(0, nz)
        def _(zz):
            r.pre[at_span(zz), :] = up_dot(close * 2, zz) + up_dot(close * 2 + 1, zz)
    with mark("dnrel0"):
        dn_relay(0)
    with mark("upfar"):
        arrived(blocks_of(4), r.r_up.at[1])
    with mark("mmfar"):
        @pl.loop(0, nz)
        def _(zz):
            low = (1 - close) * 2
            total = r.pre[at_span(zz), :] + up_dot(low, zz) + up_dot(low + 1, zz)
            r.act[at_span(zz), :] = jnp.square(jnp.maximum(total, 0.0)).astype(BF16)

    at_pair, at_same = at_z(pair), at_z(same)
    my_half = (1 - c) * close + c * (1 - close)
    ours, theirs = y == my_half, y != my_half
    first_core = c == 0

    def block_of(kind, u):
        j, part = UNITS[kind][u]
        if part == "far":
            return j, 2 * (1 - close), 2
        if part == "near":
            return j, 2 * close, 2
        return j, 0, nz

    def product(kind, u):
        j, base, n = block_of(kind, u)
        half = close if kind == "E" else 1 - close
        need = ("E", 0) if kind == "E" else ("L", j)
        if need not in seen:
            seen.add(need)
            arrived(blocks_of(3) if kind == "E" else blocks_of(1), r.r_de.at[0] if kind == "E" else r.r_dl.at[j])
        taken = jnp.concatenate(
            [at_piece(r.dn_o, half * 4 + m, j)[...] for m in range(4)], axis=0)
        total = lax.dot_general(
            r.act[pl.ds(pl.multiple_of(base * span, span), n * span), :], taken,
            (((1,), (1,)), ((), ())), preferred_element_type=F32).reshape(n, 2, rows, wide)
        here = pl.ds(base, n)
        if (kind == "E") == (now_core == 0):
            r.part[j, here] = total
        else:
            r.cs[j, here] = total.astype(BF16)
            send(r.cs.at[j, here], r.cr.at[j, here], SUM, r.r_c.at[u], at_c)

    def over(base, n, body):
        @pl.loop(0, n)
        def _(i):
            body(base + i)

    def core_sum(kind, u):
        j, base, n = block_of(kind, u)
        here = pl.ds(base, n)
        arrived(r.cr.at[j, here], r.r_c.at[u])
        if j not in Y_FIRST[kind]:
            def body(zz):
                r.xb[j, zz] = (r.part[j, zz, ox] + r.cr[j, zz, ox].astype(F32)).astype(BF16)
                r.xs[j, zz] = r.part[j, zz, x] + r.cr[j, zz, x].astype(F32)

            over(base, n, body)
            send(r.xb.at[j, here], r.xr.at[j, here], SUM, r.r_x.at[u], at_x)
        else:
            @pl.when(theirs)
            def _():
                def body(zz):
                    r.fb[j, zz] = (r.part[j, zz] + r.cr[j, zz].astype(F32)).astype(BF16)

                over(base, n, body)
                send(r.fb.at[j, here], r.fr.at[j, here], THEIRS, r.r_y.at[u], at_y)

    def first_sum(kind, u):
        j, base, n = block_of(kind, u)
        here = pl.ds(base, n)
        if j not in Y_FIRST[kind]:
            arrived(r.xr.at[j, here], r.r_x.at[u])

            @pl.when(theirs)
            def _():
                def body(zz):
                    r.yb[j, zz] = (r.xs[j, zz] + r.xr[j, zz].astype(F32)).astype(BF16)

                over(base, n, body)
                send(r.yb.at[j, here], r.yr.at[j, here], THEIRS, r.r_y.at[u], at_y)
        else:
            @pl.when(ours)
            def _():
                arrived(r.fr.at[j, here], r.r_y.at[u])

                def body(zz):
                    def whole(xx):
                        return (r.part[j, zz, xx] + r.cr[j, zz, xx].astype(F32)
                                + r.fr[j, zz, xx].astype(F32))

                    r.xb[j, zz] = whole(ox).astype(BF16)
                    r.xs[j, zz] = whole(x)

                over(base, n, body)
                send(r.xb.at[j, here], r.xr.at[j, here], OURS, r.r_x.at[u], at_x)

    def second_sum(kind, u):
        j, base, n = block_of(kind, u)
        here, part = pl.ds(base, n), UNITS[kind][u][1]

        @pl.when(ours)
        def _():
            if j in Y_FIRST[kind]:
                arrived(r.xr.at[j, here], r.r_x.at[u])
            else:
                arrived(r.yr.at[j, here], r.r_y.at[u])

            def body(zz):
                total = r.xs[j, zz] + r.xr[j, zz].astype(F32)
                if j not in Y_FIRST[kind]:
                    total = total + r.yr[j, zz].astype(F32)
                r.kept[j, zz] = total
                r.zb[j, zz] = total.astype(BF16)

            over(base, n, body)
            for m, who in ((0, across), (1, pair)):
                if part != ("near", "far")[m]:
                    send(r.zb.at[j, who], r.zr.at[j, m], OURS, r.r_z.at[j, m], at_pair)

    def cross_sum(kind, u):
        j = UNITS[kind][u][0]

        @pl.when(ours)
        def _():
            arrived(r.zr.at[j, 0], r.r_z.at[j, 0])
            total = (r.kept[j, same] + r.zr[j, 0].astype(F32)).astype(BF16)
            for cc in range(2):
                r.zc[j, cc] = total[:, cc * half_wide:(cc + 1) * half_wide]
                send(r.zc.at[j, cc], r.zx.at[j], OURS, r.r_zx.at[j], (same * 2 + x, y * 2 + cc))

    def near_sum(kind, u):
        j = UNITS[kind][u][0]

        @pl.when(ours)
        def _():
            arrived(r.zr.at[j, 1], r.r_z.at[j, 1])
            total = r.kept[j, z] + r.zr[j, 1].astype(F32)
            mine = 0 if kind == "E" else 1
            r.ho[j] = total[:, (1 - mine) * half_wide:(2 - mine) * half_wide]
            send(r.ho.at[j], r.hi.at[j], OURS, r.r_h.at[j], at_c)
            r.own[j] = total[:, mine * half_wide:(mine + 1) * half_wide]

    def last_sum(kind, j):

        def put(base):
            total = (base + r.zx[j].astype(F32)).astype(BF16)
            for xx in range(2):
                mix_o[:, xx * feat + j * fine:xx * feat + (j + 1) * fine] = total[:, xx * fine:(xx + 1) * fine]

        arrived(r.zx.at[j], r.r_zx.at[j])
        pl.when(ours)(lambda: put(r.own[j]))

        @pl.when(theirs)
        def _():
            arrived(r.hi.at[j], r.r_h.at[j])
            put(r.hi[j])

    def more_down(kind, p):
        dn_own(p)
        dn_relay(p)

    stages = dict(
        a=product, b=core_sum, c=first_sum, d=second_sum, e=cross_sum, n=near_sum, f=last_sum, D=more_down)

    seen = set()

    def program(core):
        seen.clear()
        for step in ORDER[core]:
            with mark(step):
                stages[step[0]](step[1], int(step[2]))

    def wait_sent(kind):
        lines = tally[kind] // (cols * jnp.dtype(BF16).itemsize)
        count, deep = next((lines // deep, deep) for deep in range(rows, 0, -16) if lines % deep == 0)
        done = r.xg.at[pl.ds(0, count), pl.ds(0, deep)]
        remote(done, done, kind, r.r_tc.at[0], at_x, False).wait_send()

    def run(core):
        before = dict(tally)
        program(core)
        with mark("drain"):
            for kind in (TOKEN, WEIGHT, SUM):
                wait_sent(kind)
            pl.when(central)(lambda: wait_sent(PASSED))
            pl.when(ours)(lambda: wait_sent(OURS))
            pl.when(theirs)(lambda: wait_sent(THEIRS))
        tally.clear()
        tally.update(before)

    now_core = 0
    pl.when(first_core)(lambda: run(0))
    now_core = 1
    pl.when(jnp.logical_not(first_core))(lambda: run(1))


UNITS = {
    "E": tuple((j, "all") for j in range(PIECES)),
    "L": tuple((j, "all") for j in range(PIECES - 1)) + ((PIECES - 1, "far"), (PIECES - 1, "near")),
}
Y_FIRST = {"E": (0,), "L": (0,)}
ORDER = (
    ("DE1", "aE0", "aE1", "bE0", "aE2", "bE1", "aE3", "bE2", "DE2", "aL0", "bE3", "aL1", "DE3", "cE1", "cE0",
     "cE2", "aL2", "dE1", "cE3", "aL3", "aL4", "dE2", "dE0", "dE3", "eE1", "eE2", "eE0", "eE3", "nE1", "nE2",
     "nE0", "nE3", "fE0", "fE1", "fE2", "fE3"),
    ("DL1", "aE0", "aE1", "aE2", "aE3", "aL0", "bL0", "DL2", "aL1", "bL1", "cL0", "DL3", "aL2", "bL2", "cL1",
     "aL3", "aL4", "dL0", "bL3", "cL2", "bL4", "dL1", "eL0", "cL3", "eL1", "dL2", "cL4", "dL3", "eL2", "dL4",
     "eL3", "nL0", "nL1", "nL2", "nL4", "fL0", "fL1", "fL2", "fL3"),
)


def on_device_fused(tokens, gain, up_master, down_master):
    rows, width = tokens.shape
    feat, ff = up_master.shape
    units = ff // SUB
    nz = SUB // 2
    cols = width // nz
    fine = feat // PIECES
    wide = 4 * fine
    n, pieces = len(UNITS["L"]), PIECES
    dma = pltpu.SemaphoreType.DMA
    vmem = pl.BlockSpec(memory_space=pltpu.VMEM)
    hbm = pl.BlockSpec(memory_space=pltpu.HBM)
    anywhere = pl.BlockSpec(memory_space=pl.ANY)
    arrays = dict(
        tok=((rows, width), BF16), upm=((feat, ff), F32), dnm=((feat, ff), F32),
        xg=((2 * nz * nz, rows, cols), BF16),
        up_s=((SUB, feat, units), BF16), dn_s=((SUB, feat, units), BF16),
        up_r=((nz, feat, units), BF16), dn_r=((nz, feat, units), BF16),
        pre=((SUB * rows, units), F32), act=((SUB * rows, units), BF16),
        cs=((pieces, nz, 2, rows, wide), BF16), cr=((pieces, nz, 2, rows, wide), BF16),
        part=((pieces, nz, 2, rows, wide), F32),
        xs=((pieces, nz, rows, wide), F32), xb=((pieces, nz, rows, wide), BF16), xr=((pieces, nz, rows, wide), BF16),
        yb=((pieces, nz, rows, wide), BF16), yr=((pieces, nz, rows, wide), BF16),
        fb=((pieces, nz, 2, rows, wide), BF16), fr=((pieces, nz, 2, rows, wide), BF16),
        kept=((PIECES, nz, rows, wide), F32), zb=((PIECES, nz, rows, wide), BF16),
        zc=((PIECES, 2, rows, wide // 2), BF16), zr=((PIECES, 2, rows, wide), BF16),
        zx=((PIECES, rows, wide // 2), BF16), own=((PIECES, rows, wide // 2), F32),
        ho=((PIECES, rows, wide // 2), F32), hi=((PIECES, rows, wide // 2), F32),
    )
    sems = dict(
        s_in=(3,), s_out=(6,), r_tz=(nz,), r_tx=(nz,), r_ty=(nz, 2), r_tc=(1,), r_ux=(nz,), r_up=(2,),
        r_dx=(PIECES + 1,), r_de=(1,), r_dl=(PIECES,), r_c=(n,), r_x=(n,), r_y=(n,), r_z=(PIECES, 2),
        r_zx=(PIECES,), r_h=(PIECES,),
    )
    names = list(arrays) + list(sems)
    up_s, dn_s, mixed = pl.pallas_call(
        functools.partial(fused, nz, names),
        out_shape=(
            pltpu.VMEM((SUB * feat, units), BF16),
            pltpu.VMEM((SUB * feat, units), BF16),
            pltpu.VMEM((rows, cols), BF16),
        ),
        in_specs=[hbm, vmem, hbm, hbm],
        out_specs=(vmem, vmem, vmem),
        scratch_shapes=[pltpu.VMEM(*spec) for spec in arrays.values()] + [dma(shape) for shape in sems.values()],
        compiler_params=pltpu.CompilerParams(
            collective_id=0, has_side_effects=True, vmem_limit_bytes=62873 * 2**10),
    )(tokens, gain[None, :], up_master, down_master)
    shapes = [jax.ShapeDtypeStruct(a.shape, a.dtype) for a in (up_s, dn_s, mixed)]
    up_s, dn_s, mixed = pl.pallas_call(
        write_out, out_shape=shapes, in_specs=[anywhere] * 3, out_specs=[anywhere] * 3,
        scratch_shapes=[dma((3,))],
        compiler_params=pltpu.CompilerParams(vmem_limit_bytes=2**20),
    )(up_s, dn_s, mixed)
    return up_s[None], dn_s[None], mixed


def write_out(*refs):
    copies = [pltpu.make_async_copy(refs[n], refs[3 + n], refs[6].at[n]) for n in range(3)]
    for copy in copies:
        copy.start()
    for copy in copies:
        copy.wait()


def from_partner(block, axis, bit):
    count = lax.axis_size(axis)
    route = []
    for low in range(count):
        high = low | 1 << bit
        if high != low and high < count:
            route += [(low, high), (high, low)]
    return lax.ppermute(block, axis, route)


def on_device(tokens, gain, up_master, down_master):
    fs_count = lax.axis_size("fs")
    feat_rows = up_master.shape[0]
    units = up_master.shape[1] // SUB
    groups_count = fs_count // SUB
    member = lax.axis_index("fs") % SUB
    up_round = (gain[:, None] * up_master).astype(jnp.bfloat16)
    down_round = down_master.astype(jnp.bfloat16)

    def spread(weight):
        blocks = weight.reshape(feat_rows, SUB, units).transpose(1, 0, 2)
        return jnp.broadcast_to(blocks[None], (groups_count, SUB, feat_rows, units)).reshape(
            fs_count, feat_rows, units
        )

    up_sampled, down_sampled = (
        lax.all_to_all(spread(up_round), "fs", split_axis=0, concat_axis=1, tiled=True),
        lax.all_to_all(spread(down_round), "fs", split_axis=0, concat_axis=1, tiled=True),
    )
    levels = SUB.bit_length() - 1
    bit_list = list(range(levels))
    widened = tokens.astype(jnp.float32)
    normed = (
        widened * lax.rsqrt(jnp.mean(widened * widened, axis=1, keepdims=True) + 1e-06)
    ).astype(jnp.bfloat16)
    current = normed[None]
    for bit in bit_list:
        partner = from_partner(current, "fs", bit)
        lower = member >> bit & 1 == 0
        current = jnp.where(lower, jnp.stack([current, partner]), jnp.stack([partner, current]))
    order_now = list(reversed(bit_list))
    wanted = list(range(levels - 1, -1, -1))
    perm_axes = [
        [place for place, value in enumerate(order_now) if value == target][0] for target in wanted
    ]
    current = jnp.transpose(current, perm_axes + [levels, levels + 1, levels + 2])
    gathered = current.reshape(SUB * tokens.shape[0], tokens.shape[1])
    pre_units = jnp.dot(gathered, up_sampled[0], preferred_element_type=jnp.float32)
    act_units = jnp.square(jax.nn.relu(pre_units)).astype(jnp.bfloat16)
    partial_out = lax.dot_general(
        act_units, down_sampled[0], (((1,), (1,)), ((), ())), preferred_element_type=jnp.float32
    )
    running = partial_out.reshape((2,) * levels + (tokens.shape[0], tokens.shape[1]))
    axis_bits = list(range(levels - 1, -1, -1))
    for bit in bit_list:
        position = len([value for value in axis_bits if value > bit])
        mine = member >> bit & 1
        keep = lax.dynamic_index_in_dim(running, mine, position, keepdims=False)
        other = lax.dynamic_index_in_dim(running, 1 - mine, position, keepdims=False)
        running = keep + from_partner(other, "fs", bit)
        axis_bits = [value for value in axis_bits if value != bit]
    summed = lax.psum_scatter(running, "tp", scatter_dimension=1, tiled=True)
    return (up_sampled, down_sampled, summed.astype(jnp.bfloat16))


def solution(mesh):
    placed = (P("fs", None), P("fs"), P("fs", "tp"), P("fs", "tp"))
    one_group = mesh.shape["fs"] == SUB and mesh.shape["tp"] == 4
    return jax.shard_map(
        on_device_fused if one_group else on_device,
        mesh=mesh,
        in_specs=placed,
        out_specs=(P("fs", None, "tp"), P("fs", None, "tp"), P("fs", "tp")),
        check_vma=False,
    )
```

```python
import collections
import functools
import math
import types

import jax
import jax.numpy as jnp
from jax import lax
from jax.experimental import pallas as pl
from jax.experimental.pallas import tpu as pltpu
from jax.sharding import PartitionSpec as P

SUB = 8
EPS = 1e-06
BF16 = jnp.bfloat16
F32 = jnp.float32
PIECES = 4


def fused(nz, names, tok_h, gain, upm_h, dnm_h, up_o, dn_o, mix_o, *refs):
    r = types.SimpleNamespace(**dict(zip(names, refs)))
    r.up_o, r.dn_o = up_o, dn_o
    mark = jax.named_scope
    f, t = lax.axis_index("fs"), lax.axis_index("tp")
    z, x = f // 2, f % 2
    y, c = t // 2, t % 2
    ox, oy, oc = 1 - x, 1 - y, 1 - c
    rows, width = r.tok.shape
    cols = width // nz
    feat = r.upm.shape[0]
    units = r.act.shape[1]
    fine = feat // PIECES
    wide, half_wide = 4 * fine, 2 * fine
    span = 2 * rows
    close = z // 2
    same = (z + 2) % 4
    pair = z + 1 - 2 * (z % 2)
    across = (pair + 2) % 4
    inner, outer = 2 - close, 3 * (1 - close)
    central = jnp.logical_or(z == 1, z == 2)
    at_x = (z * 2 + ox, t)
    at_y = (f, oy * 2 + c)
    at_c = (f, y * 2 + oc)

    def at_z(zz):
        return (zz * 2 + x, t)

    fetch = [pltpu.make_async_copy(src, dst, r.s_in.at[n]) for n, (src, dst) in enumerate(
        ((tok_h, r.tok), (upm_h, r.upm), (dnm_h, r.dnm)))]
    for copy in fetch:
        copy.start()

    barrier = pltpu.get_barrier_semaphore()
    def greet(dev):
        pl.semaphore_signal(barrier, inc=1, device_id=dev, device_id_type=pl.DeviceIdType.MESH)

    for dev in (at_z(pair), at_x, at_y, at_c):
        greet(dev)

    @pl.when(central)
    def _():
        greet(at_z(inner))
        greet(at_z(outer))

    tally = collections.Counter()

    def remote(src, dst, kind, rsem, dev, counted=True):
        if counted:
            tally[kind] += math.prod(src.shape) * jnp.dtype(src.dtype).itemsize
        return pltpu.make_async_remote_copy(
            src_ref=src, dst_ref=dst, send_sem=r.s_out.at[kind], recv_sem=rsem,
            device_id=dev, device_id_type=pl.DeviceIdType.MESH)

    def send(src, dst, kind, rsem, dev):
        remote(src, dst, kind, rsem, dev).start()

    def arrived(dst, rsem):
        remote(dst, dst, 0, rsem, at_x, False).wait_recv()

    def slot(q, zz, xx):
        return (q * nz + zz) * 2 + xx

    def token(q, zz, xx):
        return r.xg.at[slot(q, zz, xx)]

    def blocks_of(n):
        return r.xg.at[pl.ds(0, n)]

    def at_rows(ref, k):
        return ref.at[pl.ds(pl.multiple_of(k * feat, feat), feat), :]

    def at_piece(ref, k, p):
        return ref.at[pl.ds(pl.multiple_of(k * feat + p * fine, fine), fine), :]

    def cast(src, dst, out, factor):
        for m in range(SUB):
            block = src[:, m * units:(m + 1) * units]
            dst[m] = (block if factor is None else factor * block).astype(BF16)
        block = src[:, pl.ds(pl.multiple_of(f * units, units), units)]
        out[pl.ds(pl.multiple_of(f * feat, feat), feat), :] = (
            block if factor is None else factor * block).astype(BF16)

    with mark("norm"):
        fetch[0].wait()
        full = r.tok[...].astype(F32)
        scale = lax.rsqrt(jnp.mean(full * full, axis=1, keepdims=True) + EPS)
        for q in range(nz):
            r.xg[slot(q, z, x)] = (full[:, q * cols:(q + 1) * cols] * scale).astype(BF16)
    with mark("barrier"):
        pl.semaphore_wait(barrier, 5)

    TOKEN, WEIGHT, SUM, PASSED, OURS, THEIRS = range(6)

    def hop(q, zz, xx, rsem, dev, kind=TOKEN):
        return remote(token(q, zz, xx), token(q, zz, xx), kind, rsem, dev)

    other = oy * 2 + c
    at = dict(own=z, pair=pair, inner=inner, outer=outer)
    at_xx = dict(x=x, ox=ox)
    over_x = {w: hop(t, zz, x, r.r_tx.at[zz], at_x) for w, zz in at.items()}
    places = [(w, xx) for w in at for xx in at_xx if (w, xx) != ("own", "x")]
    over_y = {(w, xx): hop(t, at[w], at_xx[xx], r.r_ty.at[at[w], at_xx[xx]], at_y) for w, xx in places}
    over_c = {(n, w, xx): hop(q, at[w], at_xx[xx], r.r_tc.at[0], at_c)
              for n, q in enumerate((t, other)) for w, xx in places}
    passed = {w: hop(t, at[w], x, r.r_tz.at[at[w]], at_z(pair), PASSED) for w in ("inner", "outer")}

    def spread(w, xx):
        over_y[w, xx].start()
        over_c[0, w, xx].start()

    def from_z(w, relayed=False):
        arrived(token(t, at[w], x), r.r_tz.at[at[w]])
        if relayed:
            passed[w].start()
        over_x[w].start()
        spread(w, "x")

    def from_x(w):
        arrived(token(t, at[w], ox), r.r_tx.at[at[w]])
        spread(w, "ox")

    def from_y(w, xx):
        arrived(token(other, at[w], at_xx[xx]), r.r_ty.at[at[w], at_xx[xx]])
        over_c[1, w, xx].start()

    def either(when_central, when_end):
        pl.when(central)(when_central)
        pl.when(jnp.logical_not(central))(when_end)

    def up_x(zz):
        send(r.up_s.at[zz * 2 + ox], r.up_r.at[zz], WEIGHT, r.r_ux.at[zz], at_x)

    def up_own(zz, far, counted=True):
        remote(r.up_s.at[zz * 2 + x], at_rows(r.up_o, f), WEIGHT, r.r_up.at[far], at_z(zz), counted).start()

    def up_relay(zz, far):
        arrived(r.up_r.at[zz], r.r_ux.at[zz])
        send(r.up_r.at[zz], at_rows(r.up_o, z * 2 + ox), WEIGHT, r.r_up.at[far], at_z(zz))

    def slab(p):
        return pl.ds(p * fine, fine)

    def dn_x(p):
        for zz in (inner, outer):
            send(r.dn_s.at[zz * 2 + ox, slab(p)], r.dn_r.at[zz, slab(p)], WEIGHT, r.r_dx.at[p], at_x)

    def dn_own(p):
        for zz in (inner, outer):
            send(r.dn_s.at[zz * 2 + x, slab(p)], at_piece(r.dn_o, f, p), WEIGHT, r.r_dl.at[p], at_z(zz))

    def dn_relay(p):
        arrived(r.dn_r.at[pl.ds(0, 2), slab(p)], r.r_dx.at[p])
        for zz in (inner, outer):
            send(r.dn_r.at[zz, slab(p)], at_piece(r.dn_o, z * 2 + ox, p), WEIGHT, r.r_dl.at[p], at_z(zz))

    for to in (inner, pair):
        hop(t, z, x, r.r_tz.at[z], at_z(to)).start()
    over_x["own"].start()
    with mark("castup"):
        fetch[1].wait()
        cast(r.upm, r.up_s, r.up_o, jnp.transpose(gain[...]))
    up_own(pair, 0)
    up_x(pair)
    up_x(inner)
    up_own(inner, 1)
    with mark("castdn"):
        fetch[2].wait()
        cast(r.dnm, r.dn_s, r.dn_o, None)

    def central_first():
        with mark("cinner"):
            from_z("inner", True)
        with mark("couter"):
            from_z("outer", True)

    def end_first():
        with mark("epair"):
            from_z("pair")
        with mark("exz"):
            from_x("own")

    either(central_first, end_first)
    up_x(outer)

    def central_second():
        with mark("cpair"):
            from_z("pair")
        with mark("cxz"):
            from_x("own")

    pl.when(central)(central_second)
    with mark("uppair"):
        up_relay(pair, 0)
    send(r.dn_s.at[pair * 2 + x], at_rows(r.dn_o, f), WEIGHT, r.r_de.at[0], at_z(pair))
    with mark("uprelay"):
        up_relay(inner, 1)

    def central_third():
        up_own(outer, 1)
        with mark("cxinner"):
            from_x("inner")
        with mark("cxouter"):
            from_x("outer")

    def end_third():
        with mark("expair"):
            from_x("pair")
        with mark("einner"):
            from_z("inner")
        with mark("eouter"):
            from_z("outer")
        up_own(outer, 1, False)

    either(central_third, end_third)
    send(r.dn_s.at[pair * 2 + ox], r.dn_r.at[pair], WEIGHT, r.r_dx.at[PIECES], at_x)
    send(r.up_s.at[z * 2 + ox], at_rows(r.up_o, f), WEIGHT, r.r_up.at[0], at_x)
    send(r.dn_s.at[z * 2 + ox], at_rows(r.dn_o, f), WEIGHT, r.r_de.at[0], at_x)
    for p in range(PIECES):
        dn_x(p)
    with mark("uprelay"):
        up_relay(outer, 1)
    dn_own(0)

    def central_fourth():
        with mark("cxpair"):
            from_x("pair")

    def end_fourth():
        with mark("exinner"):
            from_x("inner")
        with mark("exouter"):
            from_x("outer")

    def central_fifth():
        with mark("cy"):
            for w, xx in (("inner", "x"), ("outer", "x"), ("pair", "x"), ("own", "ox"),
                          ("inner", "ox"), ("outer", "ox"), ("pair", "ox")):
                from_y(w, xx)

    def end_fifth():
        with mark("ey"):
            for w, xx in (("pair", "x"), ("own", "ox"), ("pair", "ox"), ("inner", "x"),
                          ("outer", "x"), ("inner", "ox"), ("outer", "ox")):
                from_y(w, xx)

    either(central_fourth, end_fourth)
    with mark("dnpair"):
        arrived(r.dn_r.at[pair], r.r_dx.at[PIECES])
        send(r.dn_r.at[pair], at_rows(r.dn_o, z * 2 + ox), WEIGHT, r.r_de.at[0], at_z(pair))
    either(central_fifth, end_fifth)
    with mark("toktc"):
        arrived(blocks_of(2 * (2 * nz - 1)), r.r_tc.at[0])

    def up_dot(q, zz):
        return jnp.dot(r.xg[pl.ds(slot(q, zz, 0), 2)].reshape(span, cols),
                       r.up_o[pl.ds(pl.multiple_of(q * cols, cols), cols), :],
                       preferred_element_type=F32)

    def at_span(zz):
        return pl.ds(pl.multiple_of(zz * span, span), span)

    with mark("upnear"):
        arrived(blocks_of(3), r.r_up.at[0])
    with mark("mmnear"):
        @pl.loop(0, nz)
        def _(zz):
            r.pre[at_span(zz), :] = up_dot(close * 2, zz) + up_dot(close * 2 + 1, zz)
    with mark("upfar"):
        arrived(blocks_of(4), r.r_up.at[1])
    with mark("mmfar"):
        @pl.loop(0, nz)
        def _(zz):
            low = (1 - close) * 2
            total = r.pre[at_span(zz), :] + up_dot(low, zz) + up_dot(low + 1, zz)
            r.act[at_span(zz), :] = jnp.square(jnp.maximum(total, 0.0)).astype(BF16)

    with mark("dnrel0"):
        dn_relay(0)

    at_pair = at_z(pair)
    opposite, passed_on = 3 - z, 3 - pair
    my_half = (1 - c) * close + c * (1 - close)
    ours, theirs = y == my_half, y != my_half
    first_core = c == 0

    def block_of(kind, u):
        j, part = UNITS[kind][u]
        if part == "far":
            return j, 2 * (1 - close), 2
        if part == "near":
            return j, 2 * close, 2
        return j, 0, nz

    def product(kind, u):
        j, base, n = block_of(kind, u)
        half = close if kind == "E" else 1 - close
        need = ("E", 0) if kind == "E" else ("L", j)
        if need not in seen:
            seen.add(need)
            arrived(blocks_of(3) if kind == "E" else blocks_of(1), r.r_de.at[0] if kind == "E" else r.r_dl.at[j])
        taken = jnp.concatenate(
            [at_piece(r.dn_o, half * 4 + m, j)[...] for m in range(4)], axis=0)
        total = lax.dot_general(
            r.act[pl.ds(pl.multiple_of(base * span, span), n * span), :], taken,
            (((1,), (1,)), ((), ())), preferred_element_type=F32).reshape(n, 2, rows, wide)
        here = pl.ds(base, n)
        if (kind == "E") == (now_core == 0):
            r.part[j, here] = total
        else:
            r.cs[j, here] = total.astype(BF16)
            send(r.cs.at[j, here], r.cr.at[j, here], SUM, r.r_c.at[u], at_c)

    def over(base, n, body):
        @pl.loop(0, n)
        def _(i):
            body(base + i)

    def core_sum(kind, u):
        j, base, n = block_of(kind, u)
        here = pl.ds(base, n)
        arrived(r.cr.at[j, here], r.r_c.at[u])
        if j not in Y_FIRST[kind]:
            def body(zz):
                r.xb[j, zz] = (r.part[j, zz, ox] + r.cr[j, zz, ox].astype(F32)).astype(BF16)
                r.xs[j, zz] = r.part[j, zz, x] + r.cr[j, zz, x].astype(F32)

            over(base, n, body)
            send(r.xb.at[j, here], r.xr.at[j, here], SUM, r.r_x.at[u], at_x)
        else:
            @pl.when(theirs)
            def _():
                def body(zz):
                    r.fb[j, zz] = (r.part[j, zz] + r.cr[j, zz].astype(F32)).astype(BF16)

                over(base, n, body)
                send(r.fb.at[j, here], r.fr.at[j, here], THEIRS, r.r_y.at[u], at_y)

    def first_sum(kind, u):
        j, base, n = block_of(kind, u)
        here = pl.ds(base, n)
        if j not in Y_FIRST[kind]:
            arrived(r.xr.at[j, here], r.r_x.at[u])

            @pl.when(theirs)
            def _():
                def body(zz):
                    r.yb[j, zz] = (r.xs[j, zz] + r.xr[j, zz].astype(F32)).astype(BF16)

                over(base, n, body)
                send(r.yb.at[j, here], r.yr.at[j, here], THEIRS, r.r_y.at[u], at_y)
        else:
            @pl.when(ours)
            def _():
                arrived(r.fr.at[j, here], r.r_y.at[u])

                def body(zz):
                    def whole(xx):
                        return (r.part[j, zz, xx] + r.cr[j, zz, xx].astype(F32)
                                + r.fr[j, zz, xx].astype(F32))

                    r.xb[j, zz] = whole(ox).astype(BF16)
                    r.xs[j, zz] = whole(x)

                over(base, n, body)
                send(r.xb.at[j, here], r.xr.at[j, here], OURS, r.r_x.at[u], at_x)

    def second_sum(kind, u):
        j, base, n = block_of(kind, u)
        here, part = pl.ds(base, n), UNITS[kind][u][1]

        @pl.when(ours)
        def _():
            if j in Y_FIRST[kind]:
                arrived(r.xr.at[j, here], r.r_x.at[u])
            else:
                arrived(r.yr.at[j, here], r.r_y.at[u])

            def body(zz):
                total = r.xs[j, zz] + r.xr[j, zz].astype(F32)
                if j not in Y_FIRST[kind]:
                    total = total + r.yr[j, zz].astype(F32)
                r.kept[j, zz] = total
                r.zb[j, zz] = total.astype(BF16)

            over(base, n, body)
            for m, who in ((0, passed_on), (1, pair)):
                if part != ("near", "far")[m]:
                    send(r.zb.at[j, who], r.zr.at[j, m], OURS, r.r_z.at[j, m], at_pair)

    def cross_sum(kind, u, where=None):
        j = UNITS[kind][u][0]
        here = ours if where is None else jnp.logical_and(ours, where)

        @pl.when(here)
        def _():
            arrived(r.zr.at[j, 0], r.r_z.at[j, 0])
            total = (r.kept[j, opposite] + r.zr[j, 0].astype(F32)).astype(BF16)
            for cc in range(2):
                r.zc[j, cc] = total[:, cc * half_wide:(cc + 1) * half_wide]
                remote(r.zc.at[j, cc], r.zx.at[j], OURS, r.r_zx.at[j], (opposite * 2 + x, y * 2 + cc),
                       where is not at_end).start()

    at_end = jnp.logical_not(central)

    def central_cross(kind, u):
        cross_sum(kind, u, central)

    def end_cross(kind, u):
        cross_sum(kind, u, at_end)

    def near_sum(kind, u):
        j = UNITS[kind][u][0]

        @pl.when(ours)
        def _():
            arrived(r.zr.at[j, 1], r.r_z.at[j, 1])
            total = r.kept[j, z] + r.zr[j, 1].astype(F32)
            mine = 0 if kind == "E" else 1
            r.ho[j] = total[:, (1 - mine) * half_wide:(2 - mine) * half_wide]
            send(r.ho.at[j], r.hi.at[j], OURS, r.r_h.at[j], at_c)
            r.own[j] = total[:, mine * half_wide:(mine + 1) * half_wide]

    def last_sum(kind, j):

        def put(base):
            total = (base + r.zx[j].astype(F32)).astype(BF16)
            for xx in range(2):
                mix_o[:, xx * feat + j * fine:xx * feat + (j + 1) * fine] = total[:, xx * fine:(xx + 1) * fine]

        arrived(r.zx.at[j], r.r_zx.at[j])
        pl.when(ours)(lambda: put(r.own[j]))

        @pl.when(theirs)
        def _():
            arrived(r.hi.at[j], r.r_h.at[j])
            put(r.hi[j])

    def more_down(kind, p):
        dn_own(p)
        dn_relay(p)

    stages = dict(
        a=product, b=core_sum, c=first_sum, d=second_sum, e=cross_sum, i=central_cross, o=end_cross,
        n=near_sum, f=last_sum, D=more_down)

    seen = set()

    def program(core):
        seen.clear()
        for step in ORDER[core]:
            with mark(step):
                stages[step[0]](step[1], int(step[2]))

    def wait_sent(kind):
        lines = tally[kind] // (cols * jnp.dtype(BF16).itemsize)
        count, deep = next((lines // deep, deep) for deep in range(rows, 0, -16) if lines % deep == 0)
        done = r.xg.at[pl.ds(0, count), pl.ds(0, deep)]
        remote(done, done, kind, r.r_tc.at[0], at_x, False).wait_send()

    def run(core):
        before = dict(tally)
        program(core)
        with mark("drain"):
            for kind in (TOKEN, WEIGHT, SUM):
                wait_sent(kind)
            pl.when(central)(lambda: wait_sent(PASSED))
            pl.when(ours)(lambda: wait_sent(OURS))
            pl.when(theirs)(lambda: wait_sent(THEIRS))
        tally.clear()
        tally.update(before)

    now_core = 0
    pl.when(first_core)(lambda: run(0))
    now_core = 1
    pl.when(jnp.logical_not(first_core))(lambda: run(1))


UNITS = {
    "E": tuple((j, "all") for j in range(PIECES)),
    "L": tuple((j, "all") for j in range(PIECES - 1)) + ((PIECES - 1, "far"), (PIECES - 1, "near")),
}
Y_FIRST = {"E": (1,), "L": (0,)}
ORDER = (
    ("DE1", "aE0", "aE1", "bE0", "aE2", "bE1", "aE3", "bE2", "DE2", "aL0", "bE3", "aL1", "DE3", "cE0", "cE1",
     "aL2", "cE2", "dE0", "aL3", "aL4", "cE3", "dE1", "dE2", "dE3", "eE0", "eE1", "eE2", "eE3", "nE0", "nE1",
     "nE2", "nE3", "fE0", "fE1", "fE2", "fE3"),
    ("DL1", "aE0", "aE1", "aE2", "aE3", "aL0", "bL0", "DL2", "aL1", "bL1", "cL0", "DL3", "aL2", "bL2", "cL1",
     "aL3", "bL3", "aL4", "bL4", "dL0", "dL1", "cL2", "eL0", "cL3", "eL1", "dL2", "cL4", "oL2", "dL3", "oL3",
     "dL4", "iL2", "iL3", "nL0", "nL1", "nL2", "nL4", "fL0", "fL1", "fL2", "fL3"),
)


def on_device_fused(tokens, gain, up_master, down_master):
    rows, width = tokens.shape
    feat, ff = up_master.shape
    units = ff // SUB
    nz = SUB // 2
    cols = width // nz
    fine = feat // PIECES
    wide = 4 * fine
    n, pieces = len(UNITS["L"]), PIECES
    dma = pltpu.SemaphoreType.DMA
    vmem = pl.BlockSpec(memory_space=pltpu.VMEM)
    hbm = pl.BlockSpec(memory_space=pltpu.HBM)
    anywhere = pl.BlockSpec(memory_space=pl.ANY)
    arrays = dict(
        tok=((rows, width), BF16), upm=((feat, ff), F32), dnm=((feat, ff), F32),
        xg=((2 * nz * nz, rows, cols), BF16),
        up_s=((SUB, feat, units), BF16), dn_s=((SUB, feat, units), BF16),
        up_r=((nz, feat, units), BF16), dn_r=((nz, feat, units), BF16),
        pre=((SUB * rows, units), F32), act=((SUB * rows, units), BF16),
        cs=((pieces, nz, 2, rows, wide), BF16), cr=((pieces, nz, 2, rows, wide), BF16),
        part=((pieces, nz, 2, rows, wide), F32),
        xs=((pieces, nz, rows, wide), F32), xb=((pieces, nz, rows, wide), BF16), xr=((pieces, nz, rows, wide), BF16),
        yb=((pieces, nz, rows, wide), BF16), yr=((pieces, nz, rows, wide), BF16),
        fb=((pieces, nz, 2, rows, wide), BF16), fr=((pieces, nz, 2, rows, wide), BF16),
        kept=((PIECES, nz, rows, wide), F32), zb=((PIECES, nz, rows, wide), BF16),
        zc=((PIECES, 2, rows, wide // 2), BF16), zr=((PIECES, 2, rows, wide), BF16),
        zx=((PIECES, rows, wide // 2), BF16), own=((PIECES, rows, wide // 2), F32),
        ho=((PIECES, rows, wide // 2), F32), hi=((PIECES, rows, wide // 2), F32),
    )
    sems = dict(
        s_in=(3,), s_out=(6,), r_tz=(nz,), r_tx=(nz,), r_ty=(nz, 2), r_tc=(1,), r_ux=(nz,), r_up=(2,),
        r_dx=(PIECES + 1,), r_de=(1,), r_dl=(PIECES,), r_c=(n,), r_x=(n,), r_y=(n,), r_z=(PIECES, 2),
        r_zx=(PIECES,), r_h=(PIECES,),
    )
    names = list(arrays) + list(sems)
    up_s, dn_s, mixed = pl.pallas_call(
        functools.partial(fused, nz, names),
        out_shape=(
            pltpu.VMEM((SUB * feat, units), BF16),
            pltpu.VMEM((SUB * feat, units), BF16),
            pltpu.VMEM((rows, cols), BF16),
        ),
        in_specs=[hbm, vmem, hbm, hbm],
        out_specs=(vmem, vmem, vmem),
        scratch_shapes=[pltpu.VMEM(*spec) for spec in arrays.values()] + [dma(shape) for shape in sems.values()],
        compiler_params=pltpu.CompilerParams(
            collective_id=0, has_side_effects=True, vmem_limit_bytes=62873 * 2**10),
    )(tokens, gain[None, :], up_master, down_master)
    shapes = [jax.ShapeDtypeStruct(a.shape, a.dtype) for a in (up_s, dn_s, mixed)]
    up_s, dn_s, mixed = pl.pallas_call(
        write_out, out_shape=shapes, in_specs=[anywhere] * 3, out_specs=[anywhere] * 3,
        scratch_shapes=[dma((3,))],
        compiler_params=pltpu.CompilerParams(vmem_limit_bytes=2**20),
    )(up_s, dn_s, mixed)
    return up_s[None], dn_s[None], mixed


def write_out(*refs):
    copies = [pltpu.make_async_copy(refs[n], refs[3 + n], refs[6].at[n]) for n in range(3)]
    for copy in copies:
        copy.start()
    for copy in copies:
        copy.wait()


def from_partner(block, axis, bit):
    count = lax.axis_size(axis)
    route = []
    for low in range(count):
        high = low | 1 << bit
        if high != low and high < count:
            route += [(low, high), (high, low)]
    return lax.ppermute(block, axis, route)


def on_device(tokens, gain, up_master, down_master):
    fs_count = lax.axis_size("fs")
    feat_rows = up_master.shape[0]
    units = up_master.shape[1] // SUB
    groups_count = fs_count // SUB
    member = lax.axis_index("fs") % SUB
    up_round = (gain[:, None] * up_master).astype(jnp.bfloat16)
    down_round = down_master.astype(jnp.bfloat16)

    def spread(weight):
        blocks = weight.reshape(feat_rows, SUB, units).transpose(1, 0, 2)
        return jnp.broadcast_to(blocks[None], (groups_count, SUB, feat_rows, units)).reshape(
            fs_count, feat_rows, units
        )

    up_sampled, down_sampled = (
        lax.all_to_all(spread(up_round), "fs", split_axis=0, concat_axis=1, tiled=True),
        lax.all_to_all(spread(down_round), "fs", split_axis=0, concat_axis=1, tiled=True),
    )
    levels = SUB.bit_length() - 1
    bit_list = list(range(levels))
    widened = tokens.astype(jnp.float32)
    normed = (
        widened * lax.rsqrt(jnp.mean(widened * widened, axis=1, keepdims=True) + 1e-06)
    ).astype(jnp.bfloat16)
    current = normed[None]
    for bit in bit_list:
        partner = from_partner(current, "fs", bit)
        lower = member >> bit & 1 == 0
        current = jnp.where(lower, jnp.stack([current, partner]), jnp.stack([partner, current]))
    order_now = list(reversed(bit_list))
    wanted = list(range(levels - 1, -1, -1))
    perm_axes = [
        [place for place, value in enumerate(order_now) if value == target][0] for target in wanted
    ]
    current = jnp.transpose(current, perm_axes + [levels, levels + 1, levels + 2])
    gathered = current.reshape(SUB * tokens.shape[0], tokens.shape[1])
    pre_units = jnp.dot(gathered, up_sampled[0], preferred_element_type=jnp.float32)
    act_units = jnp.square(jax.nn.relu(pre_units)).astype(jnp.bfloat16)
    partial_out = lax.dot_general(
        act_units, down_sampled[0], (((1,), (1,)), ((), ())), preferred_element_type=jnp.float32
    )
    running = partial_out.reshape((2,) * levels + (tokens.shape[0], tokens.shape[1]))
    axis_bits = list(range(levels - 1, -1, -1))
    for bit in bit_list:
        position = len([value for value in axis_bits if value > bit])
        mine = member >> bit & 1
        keep = lax.dynamic_index_in_dim(running, mine, position, keepdims=False)
        other = lax.dynamic_index_in_dim(running, 1 - mine, position, keepdims=False)
        running = keep + from_partner(other, "fs", bit)
        axis_bits = [value for value in axis_bits if value != bit]
    summed = lax.psum_scatter(running, "tp", scatter_dimension=1, tiled=True)
    return (up_sampled, down_sampled, summed.astype(jnp.bfloat16))


def solution(mesh):
    placed = (P("fs", None), P("fs"), P("fs", "tp"), P("fs", "tp"))
    one_group = mesh.shape["fs"] == SUB and mesh.shape["tp"] == 4
    return jax.shard_map(
        on_device_fused if one_group else on_device,
        mesh=mesh,
        in_specs=placed,
        out_specs=(P("fs", None, "tp"), P("fs", None, "tp"), P("fs", "tp")),
        check_vma=False,
    )
```

```python
import collections
import functools
import math
import types

import jax
import jax.numpy as jnp
from jax import lax
from jax.experimental import pallas as pl
from jax.experimental.pallas import tpu as pltpu
from jax.sharding import PartitionSpec as P

SUB = 8
EPS = 1e-06
BF16 = jnp.bfloat16
F32 = jnp.float32
PIECES = 4


def fused(nz, names, tok_h, gain, upm_h, dnm_h, up_o, dn_o, mix_o, *refs):
    r = types.SimpleNamespace(**dict(zip(names, refs)))
    r.up_o, r.dn_o = up_o, dn_o
    mark = jax.named_scope
    f, t = lax.axis_index("fs"), lax.axis_index("tp")
    z, x = f // 2, f % 2
    y, c = t // 2, t % 2
    ox, oy, oc = 1 - x, 1 - y, 1 - c
    rows, width = r.tok.shape
    cols = width // nz
    feat = r.upm.shape[0]
    units = r.act.shape[1]
    fine = feat // PIECES
    wide, half_wide = 4 * fine, 2 * fine
    span = 2 * rows
    close = z // 2
    same = (z + 2) % 4
    pair = z + 1 - 2 * (z % 2)
    across = (pair + 2) % 4
    inner, outer = 2 - close, 3 * (1 - close)
    central = jnp.logical_or(z == 1, z == 2)
    at_x = (z * 2 + ox, t)
    at_y = (f, oy * 2 + c)
    at_c = (f, y * 2 + oc)

    def at_z(zz):
        return (zz * 2 + x, t)

    fetch = [pltpu.make_async_copy(src, dst, r.s_in.at[n]) for n, (src, dst) in enumerate(
        ((tok_h, r.tok), (upm_h, r.upm), (dnm_h, r.dnm)))]
    for copy in fetch:
        copy.start()

    barrier = pltpu.get_barrier_semaphore()
    def greet(dev):
        pl.semaphore_signal(barrier, inc=1, device_id=dev, device_id_type=pl.DeviceIdType.MESH)

    for dev in (at_z(pair), at_x, at_y, at_c):
        greet(dev)

    @pl.when(central)
    def _():
        greet(at_z(inner))
        greet(at_z(outer))

    tally = collections.Counter()

    def remote(src, dst, kind, rsem, dev, counted=True):
        if counted:
            tally[kind] += math.prod(src.shape) * jnp.dtype(src.dtype).itemsize
        return pltpu.make_async_remote_copy(
            src_ref=src, dst_ref=dst, send_sem=r.s_out.at[kind], recv_sem=rsem,
            device_id=dev, device_id_type=pl.DeviceIdType.MESH)

    def send(src, dst, kind, rsem, dev):
        remote(src, dst, kind, rsem, dev).start()

    def arrived(dst, rsem):
        remote(dst, dst, 0, rsem, at_x, False).wait_recv()

    def slot(q, zz, xx):
        return (q * nz + zz) * 2 + xx

    def token(q, zz, xx):
        return r.xg.at[slot(q, zz, xx)]

    def blocks_of(n):
        return r.xg.at[pl.ds(0, n)]

    def at_rows(ref, k):
        return ref.at[pl.ds(pl.multiple_of(k * feat, feat), feat), :]

    def at_piece(ref, k, p):
        return ref.at[pl.ds(pl.multiple_of(k * feat + p * fine, fine), fine), :]

    def cast(src, dst, out, factor):
        for m in range(SUB):
            block = src[:, m * units:(m + 1) * units]
            dst[m] = (block if factor is None else factor * block).astype(BF16)
        block = src[:, pl.ds(pl.multiple_of(f * units, units), units)]
        out[pl.ds(pl.multiple_of(f * feat, feat), feat), :] = (
            block if factor is None else factor * block).astype(BF16)

    def normed(q):
        part = r.tok[:, pl.ds(pl.multiple_of(q * cols, cols), cols)].astype(F32)
        r.xg[slot(q, z, x)] = (part * scale).astype(BF16)

    with mark("norm"):
        fetch[0].wait()
        full = r.tok[...].astype(F32)
        scale = lax.rsqrt(jnp.mean(full * full, axis=1, keepdims=True) + EPS)
        normed(t)
    with mark("barrier"):
        pl.semaphore_wait(barrier, 5)

    TOKEN, WEIGHT, SUM, PASSED, OURS, THEIRS = range(6)

    def hop(q, zz, xx, rsem, dev, kind=TOKEN):
        return remote(token(q, zz, xx), token(q, zz, xx), kind, rsem, dev)

    other = oy * 2 + c
    at = dict(own=z, pair=pair, inner=inner, outer=outer)
    at_xx = dict(x=x, ox=ox)
    over_x = {w: hop(t, zz, x, r.r_tx.at[zz], at_x) for w, zz in at.items()}
    places = [(w, xx) for w in at for xx in at_xx if (w, xx) != ("own", "x")]
    over_y = {(w, xx): hop(t, at[w], at_xx[xx], r.r_ty.at[at[w], at_xx[xx]], at_y) for w, xx in places}
    over_c = {(n, w, xx): hop(q, at[w], at_xx[xx], r.r_tc.at[0], at_c)
              for n, q in enumerate((t, other)) for w, xx in places}
    passed = {w: hop(t, at[w], x, r.r_tz.at[at[w]], at_z(pair), PASSED) for w in ("inner", "outer")}

    def spread(w, xx):
        over_y[w, xx].start()
        over_c[0, w, xx].start()

    def from_z(w, relayed=False):
        arrived(token(t, at[w], x), r.r_tz.at[at[w]])
        if relayed:
            passed[w].start()
        over_x[w].start()
        spread(w, "x")

    def from_x(w):
        arrived(token(t, at[w], ox), r.r_tx.at[at[w]])
        spread(w, "ox")

    def from_y(w, xx):
        arrived(token(other, at[w], at_xx[xx]), r.r_ty.at[at[w], at_xx[xx]])
        over_c[1, w, xx].start()

    def either(when_central, when_end):
        pl.when(central)(when_central)
        pl.when(jnp.logical_not(central))(when_end)

    def up_x(zz):
        send(r.up_s.at[zz * 2 + ox], r.up_r.at[zz], WEIGHT, r.r_ux.at[zz], at_x)

    def up_own(zz, far, counted=True):
        remote(r.up_s.at[zz * 2 + x], at_rows(r.up_o, f), WEIGHT, r.r_up.at[far], at_z(zz), counted).start()

    def up_relay(zz, far):
        arrived(r.up_r.at[zz], r.r_ux.at[zz])
        send(r.up_r.at[zz], at_rows(r.up_o, z * 2 + ox), WEIGHT, r.r_up.at[far], at_z(zz))

    def slab(p):
        return pl.ds(p * fine, fine)

    def dn_x(p):
        for zz in (inner, outer):
            send(r.dn_s.at[zz * 2 + ox, slab(p)], r.dn_r.at[zz, slab(p)], WEIGHT, r.r_dx.at[p], at_x)

    def dn_own(p):
        for zz in (inner, outer):
            send(r.dn_s.at[zz * 2 + x, slab(p)], at_piece(r.dn_o, f, p), WEIGHT, r.r_dl.at[p], at_z(zz))

    def dn_relay(p):
        arrived(r.dn_r.at[pl.ds(0, 2), slab(p)], r.r_dx.at[p])
        for zz in (inner, outer):
            send(r.dn_r.at[zz, slab(p)], at_piece(r.dn_o, z * 2 + ox, p), WEIGHT, r.r_dl.at[p], at_z(zz))

    for to in (inner, pair):
        hop(t, z, x, r.r_tz.at[z], at_z(to)).start()
    over_x["own"].start()
    for step in range(1, nz):
        normed((t + step) % nz)
    with mark("castup"):
        fetch[1].wait()
        cast(r.upm, r.up_s, r.up_o, jnp.transpose(gain[...]))
    up_own(pair, 0)
    up_x(pair)
    up_x(inner)
    up_own(inner, 1)
    with mark("castdn"):
        fetch[2].wait()
        cast(r.dnm, r.dn_s, r.dn_o, None)

    def central_first():
        with mark("cinner"):
            from_z("inner", True)
        with mark("couter"):
            from_z("outer", True)

    def end_first():
        with mark("epair"):
            from_z("pair")
        with mark("exz"):
            from_x("own")

    either(central_first, end_first)
    up_x(outer)

    def central_second():
        with mark("cpair"):
            from_z("pair")
        with mark("cxz"):
            from_x("own")

    pl.when(central)(central_second)
    with mark("uppair"):
        up_relay(pair, 0)
    send(r.dn_s.at[pair * 2 + x], at_rows(r.dn_o, f), WEIGHT, r.r_de.at[0], at_z(pair))
    with mark("uprelay"):
        up_relay(inner, 1)

    def central_third():
        up_own(outer, 1)
        with mark("cxinner"):
            from_x("inner")
        with mark("cxouter"):
            from_x("outer")

    def end_third():
        with mark("expair"):
            from_x("pair")
        with mark("einner"):
            from_z("inner")
        with mark("eouter"):
            from_z("outer")
        up_own(outer, 1, False)

    either(central_third, end_third)
    send(r.dn_s.at[pair * 2 + ox], r.dn_r.at[pair], WEIGHT, r.r_dx.at[PIECES], at_x)
    send(r.up_s.at[z * 2 + ox], at_rows(r.up_o, f), WEIGHT, r.r_up.at[0], at_x)
    send(r.dn_s.at[z * 2 + ox], at_rows(r.dn_o, f), WEIGHT, r.r_de.at[0], at_x)
    for p in range(PIECES):
        dn_x(p)
    with mark("uprelay"):
        up_relay(outer, 1)
    dn_own(0)

    def central_fourth():
        with mark("cxpair"):
            from_x("pair")

    def end_fourth():
        with mark("exinner"):
            from_x("inner")
        with mark("exouter"):
            from_x("outer")

    def central_fifth():
        with mark("cy"):
            for w, xx in (("inner", "x"), ("outer", "x"), ("pair", "x"), ("own", "ox"),
                          ("inner", "ox"), ("outer", "ox"), ("pair", "ox")):
                from_y(w, xx)

    def end_fifth():
        with mark("ey"):
            for w, xx in (("pair", "x"), ("own", "ox"), ("pair", "ox"), ("inner", "x"),
                          ("outer", "x"), ("inner", "ox"), ("outer", "ox")):
                from_y(w, xx)

    either(central_fourth, end_fourth)
    with mark("dnpair"):
        arrived(r.dn_r.at[pair], r.r_dx.at[PIECES])
        send(r.dn_r.at[pair], at_rows(r.dn_o, z * 2 + ox), WEIGHT, r.r_de.at[0], at_z(pair))
    either(central_fifth, end_fifth)
    with mark("toktc"):
        arrived(blocks_of(2 * (2 * nz - 1)), r.r_tc.at[0])

    def up_dot(q, zz):
        return jnp.dot(r.xg[pl.ds(slot(q, zz, 0), 2)].reshape(span, cols),
                       r.up_o[pl.ds(pl.multiple_of(q * cols, cols), cols), :],
                       preferred_element_type=F32)

    def at_span(zz):
        return pl.ds(pl.multiple_of(zz * span, span), span)

    with mark("upnear"):
        arrived(blocks_of(3), r.r_up.at[0])
    with mark("mmnear"):
        @pl.loop(0, nz)
        def _(zz):
            r.pre[at_span(zz), :] = up_dot(close * 2, zz) + up_dot(close * 2 + 1, zz)
    with mark("upfar"):
        arrived(blocks_of(4), r.r_up.at[1])
    with mark("mmfar"):
        @pl.loop(0, nz)
        def _(zz):
            low = (1 - close) * 2
            total = r.pre[at_span(zz), :] + up_dot(low, zz) + up_dot(low + 1, zz)
            r.act[at_span(zz), :] = jnp.square(jnp.maximum(total, 0.0)).astype(BF16)

    with mark("dnrel0"):
        dn_relay(0)

    at_pair = at_z(pair)
    opposite, passed_on = 3 - z, 3 - pair
    my_half = (1 - c) * close + c * (1 - close)
    ours, theirs = y == my_half, y != my_half
    first_core = c == 0

    def block_of(kind, u):
        j, part = UNITS[kind][u]
        if part == "far":
            return j, 2 * (1 - close), 2
        if part == "near":
            return j, 2 * close, 2
        return j, 0, nz

    def product(kind, u):
        j, base, n = block_of(kind, u)
        half = close if kind == "E" else 1 - close
        need = ("E", 0) if kind == "E" else ("L", j)
        if need not in seen:
            seen.add(need)
            arrived(blocks_of(3) if kind == "E" else blocks_of(1), r.r_de.at[0] if kind == "E" else r.r_dl.at[j])
        taken = jnp.concatenate(
            [at_piece(r.dn_o, half * 4 + m, j)[...] for m in range(4)], axis=0)
        total = lax.dot_general(
            r.act[pl.ds(pl.multiple_of(base * span, span), n * span), :], taken,
            (((1,), (1,)), ((), ())), preferred_element_type=F32).reshape(n, 2, rows, wide)
        here = pl.ds(base, n)
        if (kind == "E") == (now_core == 0):
            r.part[j, here] = total
        else:
            r.cs[j, here] = total.astype(BF16)
            send(r.cs.at[j, here], r.cr.at[j, here], SUM, r.r_c.at[u], at_c)

    def over(base, n, body):
        @pl.loop(0, n)
        def _(i):
            body(base + i)

    def core_sum(kind, u):
        j, base, n = block_of(kind, u)
        here = pl.ds(base, n)
        arrived(r.cr.at[j, here], r.r_c.at[u])
        if j not in Y_FIRST[kind]:
            def body(zz):
                r.xb[j, zz] = (r.part[j, zz, ox] + r.cr[j, zz, ox].astype(F32)).astype(BF16)
                r.xs[j, zz] = r.part[j, zz, x] + r.cr[j, zz, x].astype(F32)

            over(base, n, body)
            send(r.xb.at[j, here], r.xr.at[j, here], SUM, r.r_x.at[u], at_x)
        else:
            @pl.when(theirs)
            def _():
                def body(zz):
                    r.fb[j, zz] = (r.part[j, zz] + r.cr[j, zz].astype(F32)).astype(BF16)

                over(base, n, body)
                send(r.fb.at[j, here], r.fr.at[j, here], THEIRS, r.r_y.at[u], at_y)

    def first_sum(kind, u):
        j, base, n = block_of(kind, u)
        here = pl.ds(base, n)
        if j not in Y_FIRST[kind]:
            arrived(r.xr.at[j, here], r.r_x.at[u])

            @pl.when(theirs)
            def _():
                def body(zz):
                    r.yb[j, zz] = (r.xs[j, zz] + r.xr[j, zz].astype(F32)).astype(BF16)

                over(base, n, body)
                send(r.yb.at[j, here], r.yr.at[j, here], THEIRS, r.r_y.at[u], at_y)
        else:
            @pl.when(ours)
            def _():
                arrived(r.fr.at[j, here], r.r_y.at[u])

                def body(zz):
                    def whole(xx):
                        return (r.part[j, zz, xx] + r.cr[j, zz, xx].astype(F32)
                                + r.fr[j, zz, xx].astype(F32))

                    r.xb[j, zz] = whole(ox).astype(BF16)
                    r.xs[j, zz] = whole(x)

                over(base, n, body)
                send(r.xb.at[j, here], r.xr.at[j, here], OURS, r.r_x.at[u], at_x)

    def second_sum(kind, u):
        j, base, n = block_of(kind, u)
        here, part = pl.ds(base, n), UNITS[kind][u][1]

        @pl.when(ours)
        def _():
            if j in Y_FIRST[kind]:
                arrived(r.xr.at[j, here], r.r_x.at[u])
            else:
                arrived(r.yr.at[j, here], r.r_y.at[u])

            def body(zz):
                total = r.xs[j, zz] + r.xr[j, zz].astype(F32)
                if j not in Y_FIRST[kind]:
                    total = total + r.yr[j, zz].astype(F32)
                r.kept[j, zz] = total
                r.zb[j, zz] = total.astype(BF16)

            over(base, n, body)
            for m, who in ((0, passed_on), (1, pair)):
                if part != ("near", "far")[m]:
                    send(r.zb.at[j, who], r.zr.at[j, m], OURS, r.r_z.at[j, m], at_pair)

    def cross_sum(kind, u, where=None):
        j = UNITS[kind][u][0]
        here = ours if where is None else jnp.logical_and(ours, where)

        @pl.when(here)
        def _():
            arrived(r.zr.at[j, 0], r.r_z.at[j, 0])
            total = (r.kept[j, opposite] + r.zr[j, 0].astype(F32)).astype(BF16)
            for cc in range(2):
                r.zc[j, cc] = total[:, cc * half_wide:(cc + 1) * half_wide]
                remote(r.zc.at[j, cc], r.zx.at[j], OURS, r.r_zx.at[j], (opposite * 2 + x, y * 2 + cc),
                       where is not at_end).start()

    at_end = jnp.logical_not(central)

    def central_cross(kind, u):
        cross_sum(kind, u, central)

    def end_cross(kind, u):
        cross_sum(kind, u, at_end)

    def near_sum(kind, u):
        j = UNITS[kind][u][0]

        @pl.when(ours)
        def _():
            arrived(r.zr.at[j, 1], r.r_z.at[j, 1])
            total = r.kept[j, z] + r.zr[j, 1].astype(F32)
            mine = 0 if kind == "E" else 1
            r.ho[j] = total[:, (1 - mine) * half_wide:(2 - mine) * half_wide]
            send(r.ho.at[j], r.hi.at[j], OURS, r.r_h.at[j], at_c)
            r.own[j] = total[:, mine * half_wide:(mine + 1) * half_wide]

    def last_sum(kind, j):

        def put(base):
            total = (base + r.zx[j].astype(F32)).astype(BF16)
            for xx in range(2):
                mix_o[:, xx * feat + j * fine:xx * feat + (j + 1) * fine] = total[:, xx * fine:(xx + 1) * fine]

        arrived(r.zx.at[j], r.r_zx.at[j])
        pl.when(ours)(lambda: put(r.own[j]))

        @pl.when(theirs)
        def _():
            arrived(r.hi.at[j], r.r_h.at[j])
            put(r.hi[j])

    def more_down(kind, p):
        dn_own(p)
        dn_relay(p)

    stages = dict(
        a=product, b=core_sum, c=first_sum, d=second_sum, e=cross_sum, i=central_cross, o=end_cross,
        n=near_sum, f=last_sum, D=more_down)

    seen = set()

    def program(core):
        seen.clear()
        for step in ORDER[core]:
            with mark(step):
                stages[step[0]](step[1], int(step[2]))

    def wait_sent(kind):
        lines = tally[kind] // (cols * jnp.dtype(BF16).itemsize)
        count, deep = next((lines // deep, deep) for deep in range(rows, 0, -16) if lines % deep == 0)
        done = r.xg.at[pl.ds(0, count), pl.ds(0, deep)]
        remote(done, done, kind, r.r_tc.at[0], at_x, False).wait_send()

    def run(core):
        before = dict(tally)
        program(core)
        with mark("drain"):
            for kind in (TOKEN, WEIGHT, SUM):
                wait_sent(kind)
            pl.when(central)(lambda: wait_sent(PASSED))
            pl.when(ours)(lambda: wait_sent(OURS))
            pl.when(theirs)(lambda: wait_sent(THEIRS))
        tally.clear()
        tally.update(before)

    now_core = 0
    pl.when(first_core)(lambda: run(0))
    now_core = 1
    pl.when(jnp.logical_not(first_core))(lambda: run(1))


UNITS = {
    "E": tuple((j, "all") for j in range(PIECES)),
    "L": tuple((j, "all") for j in range(PIECES - 1)) + ((PIECES - 1, "far"), (PIECES - 1, "near")),
}
Y_FIRST = {"E": (1,), "L": (0,)}
ORDER = (
    ("DE1", "aE0", "aE1", "bE0", "aE2", "bE1", "aE3", "bE2", "DE2", "aL0", "bE3", "aL1", "DE3", "cE0", "cE1",
     "aL2", "cE2", "dE0", "aL3", "aL4", "cE3", "dE1", "dE2", "dE3", "eE0", "eE1", "eE2", "eE3", "nE0", "nE1",
     "nE2", "nE3", "fE0", "fE1", "fE2", "fE3"),
    ("DL1", "aE0", "aE1", "aE2", "aL0", "aE3", "bL0", "DL2", "aL1", "bL1", "cL0", "DL3", "aL2", "bL2", "cL1",
     "aL3", "bL3", "aL4", "bL4", "dL0", "dL1", "cL2", "eL0", "cL3", "eL1", "dL2", "cL4", "oL2", "dL3", "oL3",
     "dL4", "iL2", "iL3", "nL0", "nL1", "nL2", "nL4", "fL0", "fL1", "fL2", "fL3"),
)


def on_device_fused(tokens, gain, up_master, down_master):
    rows, width = tokens.shape
    feat, ff = up_master.shape
    units = ff // SUB
    nz = SUB // 2
    cols = width // nz
    fine = feat // PIECES
    wide = 4 * fine
    n, pieces = len(UNITS["L"]), PIECES
    dma = pltpu.SemaphoreType.DMA
    vmem = pl.BlockSpec(memory_space=pltpu.VMEM)
    hbm = pl.BlockSpec(memory_space=pltpu.HBM)
    anywhere = pl.BlockSpec(memory_space=pl.ANY)
    arrays = dict(
        tok=((rows, width), BF16), upm=((feat, ff), F32), dnm=((feat, ff), F32),
        xg=((2 * nz * nz, rows, cols), BF16),
        up_s=((SUB, feat, units), BF16), dn_s=((SUB, feat, units), BF16),
        up_r=((nz, feat, units), BF16), dn_r=((nz, feat, units), BF16),
        pre=((SUB * rows, units), F32), act=((SUB * rows, units), BF16),
        cs=((pieces, nz, 2, rows, wide), BF16), cr=((pieces, nz, 2, rows, wide), BF16),
        part=((pieces, nz, 2, rows, wide), F32),
        xs=((pieces, nz, rows, wide), F32), xb=((pieces, nz, rows, wide), BF16), xr=((pieces, nz, rows, wide), BF16),
        yb=((pieces, nz, rows, wide), BF16), yr=((pieces, nz, rows, wide), BF16),
        fb=((pieces, nz, 2, rows, wide), BF16), fr=((pieces, nz, 2, rows, wide), BF16),
        kept=((PIECES, nz, rows, wide), F32), zb=((PIECES, nz, rows, wide), BF16),
        zc=((PIECES, 2, rows, wide // 2), BF16), zr=((PIECES, 2, rows, wide), BF16),
        zx=((PIECES, rows, wide // 2), BF16), own=((PIECES, rows, wide // 2), F32),
        ho=((PIECES, rows, wide // 2), F32), hi=((PIECES, rows, wide // 2), F32),
    )
    sems = dict(
        s_in=(3,), s_out=(6,), r_tz=(nz,), r_tx=(nz,), r_ty=(nz, 2), r_tc=(1,), r_ux=(nz,), r_up=(2,),
        r_dx=(PIECES + 1,), r_de=(1,), r_dl=(PIECES,), r_c=(n,), r_x=(n,), r_y=(n,), r_z=(PIECES, 2),
        r_zx=(PIECES,), r_h=(PIECES,),
    )
    names = list(arrays) + list(sems)
    up_s, dn_s, mixed = pl.pallas_call(
        functools.partial(fused, nz, names),
        out_shape=(
            pltpu.VMEM((SUB * feat, units), BF16),
            pltpu.VMEM((SUB * feat, units), BF16),
            pltpu.VMEM((rows, cols), BF16),
        ),
        in_specs=[hbm, vmem, hbm, hbm],
        out_specs=(vmem, vmem, vmem),
        scratch_shapes=[pltpu.VMEM(*spec) for spec in arrays.values()] + [dma(shape) for shape in sems.values()],
        compiler_params=pltpu.CompilerParams(
            collective_id=0, has_side_effects=True, vmem_limit_bytes=62873 * 2**10),
    )(tokens, gain[None, :], up_master, down_master)
    shapes = [jax.ShapeDtypeStruct(a.shape, a.dtype) for a in (up_s, dn_s, mixed)]
    up_s, dn_s, mixed = pl.pallas_call(
        write_out, out_shape=shapes, in_specs=[anywhere] * 3, out_specs=[anywhere] * 3,
        scratch_shapes=[dma((3,))],
        compiler_params=pltpu.CompilerParams(vmem_limit_bytes=2**20),
    )(up_s, dn_s, mixed)
    return up_s[None], dn_s[None], mixed


def write_out(*refs):
    copies = [pltpu.make_async_copy(refs[n], refs[3 + n], refs[6].at[n]) for n in range(3)]
    for copy in copies:
        copy.start()
    for copy in copies:
        copy.wait()


def from_partner(block, axis, bit):
    count = lax.axis_size(axis)
    route = []
    for low in range(count):
        high = low | 1 << bit
        if high != low and high < count:
            route += [(low, high), (high, low)]
    return lax.ppermute(block, axis, route)


def on_device(tokens, gain, up_master, down_master):
    fs_count = lax.axis_size("fs")
    feat_rows = up_master.shape[0]
    units = up_master.shape[1] // SUB
    groups_count = fs_count // SUB
    member = lax.axis_index("fs") % SUB
    up_round = (gain[:, None] * up_master).astype(jnp.bfloat16)
    down_round = down_master.astype(jnp.bfloat16)

    def spread(weight):
        blocks = weight.reshape(feat_rows, SUB, units).transpose(1, 0, 2)
        return jnp.broadcast_to(blocks[None], (groups_count, SUB, feat_rows, units)).reshape(
            fs_count, feat_rows, units
        )

    up_sampled, down_sampled = (
        lax.all_to_all(spread(up_round), "fs", split_axis=0, concat_axis=1, tiled=True),
        lax.all_to_all(spread(down_round), "fs", split_axis=0, concat_axis=1, tiled=True),
    )
    levels = SUB.bit_length() - 1
    bit_list = list(range(levels))
    widened = tokens.astype(jnp.float32)
    normed = (
        widened * lax.rsqrt(jnp.mean(widened * widened, axis=1, keepdims=True) + 1e-06)
    ).astype(jnp.bfloat16)
    current = normed[None]
    for bit in bit_list:
        partner = from_partner(current, "fs", bit)
        lower = member >> bit & 1 == 0
        current = jnp.where(lower, jnp.stack([current, partner]), jnp.stack([partner, current]))
    order_now = list(reversed(bit_list))
    wanted = list(range(levels - 1, -1, -1))
    perm_axes = [
        [place for place, value in enumerate(order_now) if value == target][0] for target in wanted
    ]
    current = jnp.transpose(current, perm_axes + [levels, levels + 1, levels + 2])
    gathered = current.reshape(SUB * tokens.shape[0], tokens.shape[1])
    pre_units = jnp.dot(gathered, up_sampled[0], preferred_element_type=jnp.float32)
    act_units = jnp.square(jax.nn.relu(pre_units)).astype(jnp.bfloat16)
    partial_out = lax.dot_general(
        act_units, down_sampled[0], (((1,), (1,)), ((), ())), preferred_element_type=jnp.float32
    )
    running = partial_out.reshape((2,) * levels + (tokens.shape[0], tokens.shape[1]))
    axis_bits = list(range(levels - 1, -1, -1))
    for bit in bit_list:
        position = len([value for value in axis_bits if value > bit])
        mine = member >> bit & 1
        keep = lax.dynamic_index_in_dim(running, mine, position, keepdims=False)
        other = lax.dynamic_index_in_dim(running, 1 - mine, position, keepdims=False)
        running = keep + from_partner(other, "fs", bit)
        axis_bits = [value for value in axis_bits if value != bit]
    summed = lax.psum_scatter(running, "tp", scatter_dimension=1, tiled=True)
    return (up_sampled, down_sampled, summed.astype(jnp.bfloat16))


def solution(mesh):
    placed = (P("fs", None), P("fs"), P("fs", "tp"), P("fs", "tp"))
    one_group = mesh.shape["fs"] == SUB and mesh.shape["tp"] == 4
    return jax.shard_map(
        on_device_fused if one_group else on_device,
        mesh=mesh,
        in_specs=placed,
        out_specs=(P("fs", None, "tp"), P("fs", None, "tp"), P("fs", "tp")),
        check_vma=False,
    )
```
